128 devices in a mesh: sp: 16 (over z, x), tp: 8 (over y, core).
Axes of the slice: x: 4, y: 4, z: 4, core: 2. Of those that a mesh axis runs over, the one named last changes fastest.
Arguments:
- inputs: bfloat16 [16384, 2048], P('sp'), may hold values from -9 to 9
- w_query: bfloat16 [2048, 1024], P(None, 'tp'), may hold values from -0.15692044 to 0.15692044
- w_key: bfloat16 [2048, 1024], P(None, 'tp'), may hold values from -0.15692044 to 0.15692044
- w_value: bfloat16 [2048, 1024], P(None, 'tp'), may hold values from -0.125 to 0.125
- w_glu_value: bfloat16 [2048, 1024], P(None, 'tp'), may hold values from -0.37565048 to 0.37565048
- w_glu_gate: bfloat16 [2048, 1024], P(None, 'tp'), may hold values from -0.125 to 0.125
- conv_taps: float32 [31, 1024], P(None, 'tp'), may hold values from -4 to 4
- conv_gain: float32 [1024], P('tp'), may hold values from 0.1 to 1.9
- log_forget: float32 [16384, 8], P('sp', 'tp'), may hold values from -16384 to 0, as said below
- w_out: bfloat16 [2048, 2048], replicated, may hold values from -0.125 to 0.125
Outputs:
- result: bfloat16 [16384, 2048], P(('sp', 'tp'))
The draws below stay inside these ranges and needn't reach their ends.
Inputs may be any that keep to these rules, and one draw needn't show every extreme that they name: `log_forget`: for each head, non-increasing along positions and at most zero.
All inputs are finite; a program needn't handle non-finite values.
Results may differ from the reference program's by a relative error of at most 0.014.
Values may be sent and summed in bfloat16 or wider, within the bound.
No kernel may reach another device: no remote copies, remote signals or barrier semaphores. Data moves between devices by JAX's collectives and lax.ppermute only.
A program may use at most 128 MiB of HBM per device.

```python
import jax
import jax.numpy as jnp
from jax import lax

D_MODEL = 2048
HEADS = 8
HEAD_DIM = 128
CONV_CH = 1024
KERNEL = 31
TOK_DEV = 1024
SEQUENCE_TOKENS = 16384


def draw_inputs(key, part):
    values = jnp.clip(jax.random.normal(jax.random.fold_in(key, 1), (SEQUENCE_TOKENS, D_MODEL), jnp.float32), -4.0, 4.0)
    return values.astype(jnp.bfloat16)


def weight_spread():
    return (3.0 / D_MODEL) ** 0.5


def query_base(key):
    return jax.random.normal(jax.random.fold_in(key, 11), (D_MODEL, HEADS * HEAD_DIM), jnp.float32) * weight_spread()


def draw_w_query(key, part):
    bound = 4.0 * weight_spread()
    return jnp.clip(query_base(key), -bound, bound).astype(jnp.bfloat16)


def draw_w_key(key, part):
    bound = 4.0 * weight_spread()
    other = jax.random.normal(jax.random.fold_in(key, 12), (D_MODEL, HEADS * HEAD_DIM), jnp.float32) * weight_spread()
    return jnp.clip(other, -bound, bound).astype(jnp.bfloat16)


def draw_w_glu_value(key, part):
    ramp = jnp.arange(CONV_CH, dtype=jnp.float32) / max(CONV_CH - 1, 1)
    shared_scale = 10.0 ** (ramp - 0.5)
    own_part = jnp.clip(jax.random.normal(jax.random.fold_in(key, 41), (D_MODEL, CONV_CH), jnp.float32), -4.0, 4.0)
    shared_column = jnp.clip(jax.random.normal(jax.random.fold_in(key, 42), (D_MODEL, 1), jnp.float32), -4.0, 4.0)
    values = (own_part + shared_scale[None, :] * shared_column) * D_MODEL ** (-0.5)
    return values.astype(jnp.bfloat16)


def draw_conv_taps(key, part):
    ramp = jnp.arange(CONV_CH, dtype=jnp.float32) / max(CONV_CH - 1, 1)
    raw = jnp.clip(jax.random.normal(jax.random.fold_in(key, 21), (KERNEL, CONV_CH), jnp.float32), -5.0, 5.0)
    scales = 10.0 ** (0.8 * ramp - 0.4)
    return (raw + 1.0) * scales[None, :] * KERNEL ** (-0.5)


def draw_log_forget(key, part):
    ranks = jax.random.permutation(jax.random.fold_in(key, 31), HEADS)
    fast_count = HEADS // 2
    is_fast = ranks < fast_count
    fast_rate = 1.0 / jax.random.uniform(jax.random.fold_in(key, 32), (HEADS,), jnp.float32, 30.0, 100.0)
    slow_total = jnp.exp(jax.random.uniform(jax.random.fold_in(key, 33), (HEADS,), jnp.float32, jnp.log(0.3), jnp.log(1.0)))
    decay_rate = jnp.where(is_fast, fast_rate, slow_total / SEQUENCE_TOKENS)
    block_count = SEQUENCE_TOKENS // TOK_DEV
    block_multiplier = jnp.exp(jax.random.uniform(jax.random.fold_in(key, 34), (block_count,), jnp.float32, jnp.log(0.5), jnp.log(2.0)))
    block_multiplier = jnp.repeat(block_multiplier, TOK_DEV)
    coarse_estimate = jax.random.uniform(jax.random.fold_in(key, 35), (SEQUENCE_TOKENS, HEADS), jnp.float32, 0.2, 1.8)
    spike_position = jax.random.randint(jax.random.fold_in(key, 36), (3,), 0, SEQUENCE_TOKENS)
    spike_loss = jax.random.uniform(jax.random.fold_in(key, 37), (3,), jnp.float32, 0.2, 0.4)
    spike_list = jnp.zeros((SEQUENCE_TOKENS,), jnp.float32).at[spike_position].add(jnp.log(1.0 - spike_loss))
    step_count = -decay_rate[None, :] * coarse_estimate * block_multiplier[:, None] + spike_list[:, None]
    return jnp.cumsum(step_count, axis=0)


def block_levels(stream_key, dims, pieces, smallest, high):
    factor_of = 1.0
    for position, shards_of in pieces:
        draws = jax.random.uniform(jax.random.fold_in(jax.random.fold_in(stream_key, 6), position), (shards_of,), jnp.float32, smallest / len(pieces), high / len(pieces))
        factor_of = factor_of * jnp.repeat(jnp.exp(draws), dims[position] // shards_of).reshape((-1,) + (1,) * (len(dims) - 1 - position))
    return factor_of


def noise(stream_key, dims, deviation, reach, pieces=(), kind=jnp.bfloat16):
    drawn = deviation * jax.random.normal(stream_key, dims, jnp.float32)
    if pieces:
        drawn = drawn * block_levels(stream_key, dims, pieces, -0.22, 0.18)
    return jnp.clip(drawn, -reach, reach).astype(kind)


def setup_inputs(seed: int = 0) -> dict:
    arg_keys = jax.random.split(jax.random.key(seed), 11)
    inputs = draw_inputs(jax.random.fold_in(arg_keys[10], 71), 0)
    w_query = draw_w_query(jax.random.fold_in(arg_keys[10], 71), 0)
    w_key = draw_w_key(jax.random.fold_in(arg_keys[10], 71), 0)
    w_value = noise(arg_keys[3], (D_MODEL, HEADS * HEAD_DIM), D_MODEL ** -0.5, 0.125, ((1, 8),))
    w_glu_value = draw_w_glu_value(jax.random.fold_in(arg_keys[10], 71), 0)
    w_glu_gate = noise(arg_keys[5], (D_MODEL, CONV_CH), D_MODEL ** -0.5, 0.125, ((1, 8),))
    conv_taps = draw_conv_taps(jax.random.fold_in(arg_keys[10], 71), 0)
    conv_gain = jnp.clip(1.0 + 0.18 * jax.random.normal(arg_keys[7], (CONV_CH,), jnp.float32), 0.1, 1.9)
    log_forget = draw_log_forget(jax.random.fold_in(arg_keys[10], 71), 0)
    w_out = noise(arg_keys[9], (CONV_CH + HEADS * HEAD_DIM, D_MODEL), (CONV_CH + HEADS * HEAD_DIM) ** -0.5, 0.125)
    return dict(inputs=inputs, w_query=w_query, w_key=w_key, w_value=w_value, w_glu_value=w_glu_value, w_glu_gate=w_glu_gate, conv_taps=conv_taps, conv_gain=conv_gain, log_forget=log_forget, w_out=w_out)


NORM_EPS = 1e-05

def reference(inputs, w_query, w_key, w_value, w_glu_value, w_glu_gate, conv_taps, conv_gain, log_forget, w_out):
    glu_value = jnp.dot(inputs, w_glu_value, preferred_element_type=jnp.float32)
    glu_gate = jnp.dot(inputs, w_glu_gate, preferred_element_type=jnp.float32)
    gated = (glu_value * jax.nn.sigmoid(glu_gate)).astype(jnp.bfloat16)
    padded = jnp.concatenate([jnp.zeros((KERNEL - 1, CONV_CH), jnp.bfloat16), gated], axis=0).astype(jnp.float32)
    conv_sum = jnp.zeros((SEQUENCE_TOKENS, CONV_CH), jnp.float32)
    for offset in range(KERNEL):
        conv_sum = conv_sum + conv_taps[offset] * padded[offset:offset + SEQUENCE_TOKENS]
    mean_value = lax.optimization_barrier(jnp.mean(conv_sum, axis=1, keepdims=True))
    centered = conv_sum - mean_value
    spread = lax.optimization_barrier(jnp.mean(centered * centered, axis=1, keepdims=True))
    conv_rows = jax.nn.silu(centered * lax.rsqrt(spread + NORM_EPS) * conv_gain).astype(jnp.bfloat16)
    query_rows = jnp.dot(inputs, w_query, preferred_element_type=jnp.float32).astype(jnp.bfloat16)
    key_rows = jnp.dot(inputs, w_key, preferred_element_type=jnp.float32).astype(jnp.bfloat16)
    value_rows = jnp.dot(inputs, w_value, preferred_element_type=jnp.float32).astype(jnp.bfloat16)
    blocks = SEQUENCE_TOKENS // TOK_DEV
    query_heads = query_rows.reshape(SEQUENCE_TOKENS, HEADS, HEAD_DIM).transpose(1, 0, 2).reshape(HEADS, blocks, TOK_DEV, HEAD_DIM)
    key_heads = key_rows.reshape(SEQUENCE_TOKENS, HEADS, HEAD_DIM).transpose(1, 0, 2)
    value_heads = value_rows.reshape(SEQUENCE_TOKENS, HEADS, HEAD_DIM).transpose(1, 0, 2)
    gate_heads = jnp.transpose(log_forget)
    gate_blocks = gate_heads.reshape(HEADS, blocks, TOK_DEV)
    positions = jnp.arange(SEQUENCE_TOKENS, dtype=jnp.int32)
    block_starts = jnp.arange(blocks, dtype=jnp.int32) * TOK_DEV
    score_scale = HEAD_DIM ** (-0.5)

    def head_output(packed):
        head_query, head_key, head_value, head_gate, head_gate_blocks = packed

        def block_output(block_packed):
            block_query, block_gate, block_start = block_packed
            scores = jnp.dot(block_query, head_key.T, preferred_element_type=jnp.float32) * score_scale
            scores = scores + block_gate[:, None] - head_gate[None, :]
            query_pos = block_start + jnp.arange(TOK_DEV, dtype=jnp.int32)
            allowed = positions[None, :] <= query_pos[:, None]
            scores = jnp.where(allowed, scores, -jnp.inf)
            row_max = lax.optimization_barrier(jnp.max(scores, axis=1, keepdims=True))
            weights = jnp.exp(scores - row_max)
            denominators = lax.optimization_barrier(jnp.sum(weights, axis=1, keepdims=True))
            mixture = jnp.dot(weights.astype(jnp.bfloat16), head_value, preferred_element_type=jnp.float32)
            return (mixture / denominators).astype(jnp.bfloat16)
        return lax.map(block_output, (head_query, head_gate_blocks, block_starts))
    attn_heads = lax.map(head_output, (query_heads, key_heads, value_heads, gate_heads, gate_blocks))
    attn_rows = attn_heads.reshape(HEADS, SEQUENCE_TOKENS, HEAD_DIM).transpose(1, 0, 2).reshape(SEQUENCE_TOKENS, HEADS * HEAD_DIM)
    projected = jnp.dot(conv_rows, w_out[:CONV_CH], preferred_element_type=jnp.float32)
    projected = projected + jnp.dot(attn_rows, w_out[CONV_CH:], preferred_element_type=jnp.float32)
    return projected.astype(jnp.bfloat16)
```

```python
import functools

import jax
import jax.numpy as jnp
import numpy as np
from jax import lax
from jax.experimental import pallas as pl
from jax.experimental.pallas import tpu as pltpu
from jax.sharding import PartitionSpec as P


BF16, F32, I32 = jnp.bfloat16, jnp.float32, jnp.int32
SIDE = 4
HEAD = 128
TOK = 1024
HALF = 512
TAPS = 31
GATE_ROW = TOK
QUERY_ROW = TOK + 16
PACK_ROWS = QUERY_ROW + HALF // 2
BACK_ROWS = HALF + 16
TILES = 15
LOG2E = 1.4426950408889634
SCALE = HEAD**-0.5 * LOG2E
LOW = -1e30
TINY = 1e-37
EPS = 1e-05

VM = pl.BlockSpec(memory_space=pltpu.VMEM)
SM = pl.BlockSpec(memory_space=pltpu.SMEM)
ANY = pl.BlockSpec(memory_space=pl.ANY)


def dot(a, b):
    return jnp.dot(a, b, preferred_element_type=F32)


def params(mib):
    return pltpu.CompilerParams(vmem_limit_bytes=mib << 20)


def cost(flops, moved):
    return pl.CostEstimate(flops=flops, bytes_accessed=moved, transcendentals=0)


def moves(dx, dz):
    return [
        (z * SIDE + x, (z + dz) % SIDE * SIDE + (x + dx) % SIDE)
        for z in range(SIDE)
        for x in range(SIDE)
    ]


def eye():
    return lax.broadcasted_iota(I32, (128, 128), 0) == lax.broadcasted_iota(I32, (128, 128), 1)


def to_row(column):
    return jnp.sum(jnp.where(eye(), column, 0.0), axis=0, keepdims=True)


def to_column(row):
    return jnp.sum(jnp.where(eye(), row, 0.0), axis=1, keepdims=True)


def split3(value):
    top = value.astype(BF16)
    rest = value - top.astype(F32)
    mid = rest.astype(BF16)
    return top, mid, (rest - mid.astype(F32)).astype(BF16)


def work_table():
    table = np.zeros((SIDE * SIDE, 2, TILES + 1), np.int32)
    for z in range(SIDE):
        for x in range(SIDE):
            tiles = []
            for d in range(SIDE):
                for e in range(SIDE):
                    late = (d == 2) + (e == 2)
                    first_z = (z + e) % SIDE
                    if first_z < z or (e == 0 and x < (x + d) % SIDE):
                        tiles.append((late, d, 3 + e if e else 0))
                    second_z = (z + d) % SIDE
                    if second_z > z or (d == 0 and (x + e) % SIDE < x):
                        tiles.append((late, 4 + d, e))
            assert len(tiles) == TILES
            for n, (_, q, k) in enumerate(sorted(tiles)):
                table[z * SIDE + x, :, n] = q, k
    return table


def project_kernel(x_hbm, wq, wk, wv, gate, px, pz, x, w, sems):
    copies = [
        pltpu.make_async_copy(
            x_hbm.at[pl.ds(256 * i, 256)], x.at[pl.ds(256 * i, 256)], sems.at[i]
        )
        for i in range(4)
    ]
    for c in copies:
        c.start()
    w[:, 0:128] = wk[...]
    w[:, 128:256] = wv[...]
    w[:, 256:384] = wq[...]
    zero = jnp.zeros((8, 128), BF16)
    scaled = jnp.concatenate(
        [to_row(gate[128 * r : 128 * r + 128, :] * (-LOG2E)) for r in range(8)], axis=0
    )
    top, mid, low = split3(scaled)
    gates = jnp.concatenate(
        [jnp.concatenate([top, mid], axis=1), jnp.concatenate([low, zero], axis=1)], axis=0
    )
    px[GATE_ROW : GATE_ROW + 16, :] = gates
    pz[GATE_ROW : GATE_ROW + 16, :] = gates
    for i in range(4):
        copies[i].wait()
        out = dot(x[256 * i : 256 * i + 256, :], w[...]).astype(BF16)
        px[256 * i : 256 * i + 256, :] = out[:, :256]
        pz[256 * i : 256 * i + 256, :] = out[:, :256]
        dest = px if i < 2 else pz
        lane = 128 * (i % 2)
        dest[QUERY_ROW:PACK_ROWS, lane : lane + 128] = out[:, 256:]


def project(x, wq, wk, wv, gate):
    pack = jax.ShapeDtypeStruct((PACK_ROWS, 256), BF16)
    return pl.pallas_call(
        project_kernel,
        out_shape=(pack, pack),
        in_specs=[ANY, VM, VM, VM, VM],
        out_specs=(VM, VM),
        scratch_shapes=[
            pltpu.VMEM((TOK, 2048), BF16),
            pltpu.VMEM((2048, 384), BF16),
            pltpu.SemaphoreType.DMA((4,)),
        ],
        compiler_params=params(32),
        cost_estimate=cost(2 * TOK * 2048 * 512, 8 << 20),
        name="project",
    )(x, wq, wk, wv, gate)


def glu_kernel(x_hbm, wu, wg, out, x, w, sems):
    copies = [
        pltpu.make_async_copy(
            x_hbm.at[pl.ds(256 * i, 256)], x.at[pl.ds(256 * i, 256)], sems.at[i]
        )
        for i in range(4)
    ]
    for c in copies:
        c.start()
    w[:, 0:128] = wu[...]
    w[:, 128:256] = wg[...]
    for i in range(4):
        copies[i].wait()
        both = dot(x[256 * i : 256 * i + 256, :], w[...])
        out[256 * i : 256 * i + 256, :] = (both[:, :128] * jax.nn.sigmoid(both[:, 128:])).astype(
            BF16
        )


def glu(x, wu, wg):
    return pl.pallas_call(
        glu_kernel,
        out_shape=jax.ShapeDtypeStruct((TOK, 128), BF16),
        in_specs=[ANY, VM, VM],
        out_specs=VM,
        scratch_shapes=[
            pltpu.VMEM((TOK, 2048), BF16),
            pltpu.VMEM((2048, 256), BF16),
            pltpu.SemaphoreType.DMA((4,)),
        ],
        compiler_params=params(32),
        cost_estimate=cost(2 * TOK * 2048 * 256, 6 << 20),
        name="glu",
    )(x, wu, wg)


def conv_kernel(gated, halo, taps, gain, out, padded):
    padded[0:32, :] = halo[...].astype(F32)
    padded[32 : 32 + TOK, :] = gated[...].astype(F32)
    padded[32 + TOK :, :] = jnp.zeros((8, 128), F32)
    for block in range(8):
        start = 128 * block
        total = None
        for r in range(8):
            part = None
            for q in range(5):
                j = 8 * q + r - 2
                if 0 <= j < TAPS:
                    term = taps[j : j + 1, :] * padded[start + 8 * q : start + 8 * q + 136, :]
                    part = term if part is None else part + term
            part = part[r : r + 128, :]
            total = part if total is None else total + part
        out[block, 0:128, :] = total
        out[block, 128:136, :] = jnp.broadcast_to(gain[...], (8, 128))


def convolve(gated, halo, taps, gain):
    return pl.pallas_call(
        conv_kernel,
        out_shape=jax.ShapeDtypeStruct((8, 136, 128), F32),
        in_specs=[VM] * 4,
        out_specs=VM,
        scratch_shapes=[pltpu.VMEM((TOK + 40, 128), F32)],
        compiler_params=params(8),
        cost_estimate=cost(2 * TOK * 128 * 31 * 64, 1 << 20),
        name="convolve",
    )(gated, halo, taps, gain)


def diagonal_kernel(px, pz, m_out, l_out, acc_out):
    top = px[GATE_ROW : GATE_ROW + 8, :].astype(F32)
    low = px[GATE_ROW + 8 : GATE_ROW + 16, :].astype(F32)
    gates = top[:, :128] + top[:, 128:] + low[:, :128]
    for half, pack in ((0, px), (1, pz)):
        keys = HALF * (half + 1)
        query = jnp.concatenate(
            [pack[QUERY_ROW:PACK_ROWS, :128], pack[QUERY_ROW:PACK_ROWS, 128:]], axis=0
        )
        scores = lax.dot_general(
            query, px[:keys, :128], (((1,), (1,)), ((), ())), preferred_element_type=F32
        )
        row = lax.broadcasted_iota(I32, (HALF, 128), 0) + HALF * half
        lane = lax.broadcasted_iota(I32, (HALF, 128), 1)
        parts = []
        for c in range(keys // 128):
            t = scores[:, 128 * c : 128 * c + 128] * SCALE + gates[c : c + 1, :]
            parts.append(jnp.where(lane + 128 * c <= row, t, LOW))
        most = functools.reduce(jnp.maximum, parts)
        most = jnp.broadcast_to(jnp.max(most, axis=1, keepdims=True), (HALF, 128))
        weights = [jnp.exp2(t - most) for t in parts]
        m_out[half] = most
        l_out[half] = functools.reduce(jnp.add, weights)
        acc_out[half] = dot(
            jnp.concatenate([w.astype(BF16) for w in weights], axis=1), px[:keys, 128:]
        )


def diagonal(px, pz):
    state = jax.ShapeDtypeStruct((2, HALF, 128), F32)
    return pl.pallas_call(
        diagonal_kernel,
        out_shape=(state, state, state),
        in_specs=[VM, VM],
        out_specs=(VM, VM, VM),
        compiler_params=params(32),
        cost_estimate=cost(2 * HALF * 2048 * 512, 4 << 20),
        name="diagonal",
    )(px, pz)


def attend_kernel(
    table, own, px, x1, x2, x3, pz, z1, z2, z3, m_in, l_in, acc_in,
    o_own, lse_own, a1, a2, a3, b1, b2, b3,
    packs, query, gates, sa, sb, ma, mb, aa, ab, m, l, acc, sems,
):
    sources = (px, x1, x2, x3, z1, z2, z3)
    copies = [
        pltpu.make_async_copy(source, packs.at[n], sems.at[n]) for n, source in enumerate(sources)
    ]
    copies.append(pltpu.make_async_copy(pz, packs.at[7], sems.at[7]))
    for c in copies:
        c.start()
    m[...] = jnp.full_like(m, LOW)
    l[...] = jnp.zeros_like(l)
    acc[...] = jnp.zeros_like(acc)
    for half in range(2):
        m[4 * half] = m_in[half]
        l[4 * half] = l_in[half]
        acc[4 * half] = acc_in[half]
    for c in copies:
        c.wait()
    for n, slot in enumerate((0, 1, 2, 3, 7, 4, 5, 6)):
        for side in range(2):
            query[n, 256 * side : 256 * side + 256, :] = packs[
                slot, QUERY_ROW:PACK_ROWS, 128 * side : 128 * side + 128
            ]
    for n in range(7):
        top = packs[n, GATE_ROW : GATE_ROW + 8, :].astype(F32)
        low = packs[n, GATE_ROW + 8 : GATE_ROW + 16, :].astype(F32)
        gates[n] = top[:, :128] + top[:, 128:] + low[:, :128]
    row = own[0]

    def scores_of(n, s, most, shrink):
        q, k = table[row, 0, n], table[row, 1, n]
        raw = lax.dot_general(
            query[q], packs[k, :TOK, :128], (((1,), (1,)), ((), ())), preferred_element_type=F32
        )
        best = None
        for c in range(8):
            t = raw[:, 128 * c : 128 * c + 128] * SCALE + gates[k, c : c + 1, :]
            s[:, 128 * c : 128 * c + 128] = t
            best = t if best is None else jnp.maximum(best, t)
        old = m[q]
        new = jnp.maximum(old, jnp.max(best, axis=1, keepdims=True))
        shrink[...] = jnp.exp2(old - new)
        m[q] = new
        most[...] = new

    def weigh(n, s, most, shrink):
        q, k = table[row, 0, n], table[row, 1, n]
        top = most[...]
        by = shrink[...]
        w = [jnp.exp2(s[:, 128 * c : 128 * c + 128] - top) for c in range(8)]
        total = ((w[0] + w[1]) + (w[2] + w[3])) + ((w[4] + w[5]) + (w[6] + w[7]))
        rounded = jnp.concatenate([v.astype(BF16) for v in w], axis=1)
        l[q] = l[q] * by + total
        acc[q] = acc[q] * by + dot(rounded, packs[k, :TOK, 128:])

    first, second = (sa, ma, aa), (sb, mb, ab)
    scores_of(0, *first)

    def two_tiles(i, carry):
        scores_of(2 * i + 1, *second)
        weigh(2 * i, *first)
        scores_of(2 * i + 2, *first)
        weigh(2 * i + 1, *second)
        return carry

    lax.fori_loop(0, (TILES - 1) // 2, two_tiles, 0)
    weigh(TILES - 1, *first)
    for n, out in enumerate((None, a1, a2, a3, None, b1, b2, b3)):
        total = jnp.maximum(jnp.sum(l[n], axis=1, keepdims=True), TINY)
        mixed = acc[n] / total
        lse = m[n] + jnp.log2(total)
        if out is None:
            o_own[n // 4] = mixed
            lse_own[n // 4] = lse
        else:
            out[0:HALF, :] = mixed.astype(BF16)
            rows = [to_row(lse[128 * b : 128 * b + 128, :]) for b in range(4)]
            parts = split3(jnp.concatenate(rows + rows, axis=0))
            out[HALF : HALF + 16, :] = jnp.concatenate(
                [parts[0][:4], parts[1][:4], parts[2]], axis=0
            )


def attend(table, own, packs, state):
    back = jax.ShapeDtypeStruct((BACK_ROWS, 128), BF16)
    kept = jax.ShapeDtypeStruct((2, HALF, 128), F32)
    per_tile = [pltpu.VMEM((HALF, 128), F32)] * 4
    return pl.pallas_call(
        attend_kernel,
        out_shape=(kept, kept) + (back,) * 6,
        in_specs=[SM, SM] + [ANY] * 8 + [VM] * 3,
        out_specs=(VM,) * 8,
        scratch_shapes=[
            pltpu.VMEM((8, PACK_ROWS, 256), BF16),
            pltpu.VMEM((8, HALF, 128), BF16),
            pltpu.VMEM((7, 8, 128), F32),
            pltpu.VMEM((HALF, TOK), F32),
            pltpu.VMEM((HALF, TOK), F32),
            *per_tile,
            *[pltpu.VMEM((8, HALF, 128), F32)] * 3,
            pltpu.SemaphoreType.DMA((8,)),
        ],
        compiler_params=params(40),
        cost_estimate=cost(TILES * 4 * HALF * TOK * 256, 8 << 20),
        name="attend",
    )(table, own, *packs, *state)


def combine_kernel(o_own, lse_own, a1, a2, a3, b1, b2, b3, out):
    for half, backs in ((0, (a1, a2, a3)), (1, (b1, b2, b3))):
        lses = []
        for back in backs:
            tail = back[HALF : HALF + 16, :].astype(F32)
            lses.append(tail[0:4] + tail[4:8] + tail[8:12])
        for b in range(4):
            rows = slice(128 * b, 128 * b + 128)
            columns = [lse_own[half, rows, :]]
            columns += [jnp.broadcast_to(to_column(v[b : b + 1, :]), (128, 128)) for v in lses]
            most = functools.reduce(jnp.maximum, columns)
            shares = [jnp.exp2(c - most) for c in columns]
            mixed = shares[0] * o_own[half, rows, :]
            for share, back in zip(shares[1:], backs):
                mixed = mixed + share * back[rows, :].astype(F32)
            out[4 * half + b] = (mixed / functools.reduce(jnp.add, shares)).astype(BF16)


def combine(o_own, lse_own, backs):
    return pl.pallas_call(
        combine_kernel,
        out_shape=jax.ShapeDtypeStruct((8, 128, 128), BF16),
        in_specs=[VM] * 8,
        out_specs=VM,
        compiler_params=params(16),
        cost_estimate=cost(1 << 29, 2 << 20),
        name="combine",
    )(o_own, lse_own, *backs)


def conv_out_kernel(parts, w, out, rows):
    @pl.when(pl.program_id(0) == 0)
    def _():
        total = functools.reduce(jnp.add, [parts[c, :128, :] for c in range(8)])
        mean = jnp.sum(total, axis=1, keepdims=True) * (1.0 / 1024)
        far = [parts[c, :128, :] - mean for c in range(8)]
        spread = functools.reduce(jnp.add, [v * v for v in far])
        spread = jnp.sum(spread, axis=1, keepdims=True) * (1.0 / 1024)
        inverse = lax.rsqrt(spread + EPS)
        for c in range(8):
            v = far[c] * inverse * parts[c, 128:129, :]
            rows[:, 128 * c : 128 * c + 128] = (v * jax.nn.sigmoid(v)).astype(BF16)

    out[...] = dot(rows[...], w[...])


def conv_out(parts, w):
    return pl.pallas_call(
        conv_out_kernel,
        grid=(4,),
        out_shape=jax.ShapeDtypeStruct((128, 2048), F32),
        in_specs=[
            pl.BlockSpec((8, 136, 128), lambda j: (0, 0, 0)),
            pl.BlockSpec((1024, 512), lambda j: (0, j)),
        ],
        out_specs=pl.BlockSpec((128, 512), lambda j: (0, j)),
        scratch_shapes=[pltpu.VMEM((128, 1024), BF16)],
        compiler_params=params(16),
        cost_estimate=cost(2 * 128 * 1024 * 2048 * 4, 6 << 20),
        name="conv_out",
    )(parts, w)


def attn_out_kernel(parts, conv, w, out, rows):
    @pl.when(pl.program_id(0) == 0)
    def _():
        for c in range(8):
            rows[:, 128 * c : 128 * c + 128] = parts[c]

    out[...] = (dot(rows[...], w[...]) + conv[...]).astype(BF16)


def attn_out(parts, conv, w):
    return pl.pallas_call(
        attn_out_kernel,
        grid=(4,),
        out_shape=jax.ShapeDtypeStruct((128, 2048), BF16),
        in_specs=[
            pl.BlockSpec((8, 128, 128), lambda j: (0, 0, 0)),
            pl.BlockSpec((128, 512), lambda j: (0, j)),
            pl.BlockSpec((1024, 512), lambda j: (1, j)),
        ],
        out_specs=pl.BlockSpec((128, 512), lambda j: (0, j)),
        scratch_shapes=[pltpu.VMEM((128, 1024), BF16)],
        compiler_params=params(16),
        cost_estimate=cost(2 * 128 * 1024 * 2048 * 4, 6 << 20),
        name="attn_out",
    )(parts, conv, w)


def on_device(x, wq, wk, wv, wu, wg, taps, gain, gate, w_out):
    own = lax.axis_index("sp").astype(I32).reshape(1)
    table = jnp.asarray(work_table())
    px, pz = project(x, wq, wk, wv, gate)
    xs, zs = [None] * 4, [None] * 4
    for d in (1, 3, 2):
        xs[d] = lax.ppermute(px, "sp", moves(-d, 0))
        zs[d] = lax.ppermute(pz, "sp", moves(0, -d))
    gated = glu(x, wu, wg)
    halo = lax.ppermute(gated[TOK - 32 :], "sp", [(i, i + 1) for i in range(15)])
    state = diagonal(px, pz)
    conv = convolve(gated, halo, taps, gain.reshape(1, 128))
    conv_parts = lax.all_to_all(conv, "tp", 0, 0, tiled=True)
    conv_mixed = conv_out(conv_parts, w_out)
    packs = (px, *xs[1:], pz, *zs[1:])
    o_own, lse_own, *sent = attend(table, own, packs, state)
    backs = [lax.ppermute(sent[d - 1], "sp", moves(d, 0)) for d in (1, 2, 3)]
    backs += [lax.ppermute(sent[d + 2], "sp", moves(0, d)) for d in (1, 2, 3)]
    mixed = combine(o_own, lse_own, backs)
    attn_parts = lax.all_to_all(mixed, "tp", 0, 0, tiled=True)
    return attn_out(attn_parts, conv_mixed, w_out)


def solution(mesh):
    in_specs = (
        P("sp", None),
        P(None, "tp"),
        P(None, "tp"),
        P(None, "tp"),
        P(None, "tp"),
        P(None, "tp"),
        P(None, "tp"),
        P("tp"),
        P("sp", "tp"),
        P(),
    )
    out_specs = P(("sp", "tp"), None)
    return jax.shard_map(
        on_device, mesh=mesh, in_specs=in_specs, out_specs=out_specs, check_vma=False
    )
```

```python
import functools

import jax
import jax.numpy as jnp
import numpy as np
from jax import lax
from jax.experimental import pallas as pl
from jax.experimental.pallas import tpu as pltpu
from jax.sharding import PartitionSpec as P


BF16, F32, I32 = jnp.bfloat16, jnp.float32, jnp.int32
SIDE = 4
HEAD = 128
TOK = 1024
HALF = 512
TAPS = 31
GATE_ROW = TOK
QUERY_ROW = TOK + 16
PACK_ROWS = QUERY_ROW + HALF // 2
BACK_ROWS = HALF + 16
TILES = 15
LOG2E = 1.4426950408889634
SCALE = HEAD**-0.5 * LOG2E
LOW = -1e30
TINY = 1e-37
EPS = 1e-05

VM = pl.BlockSpec(memory_space=pltpu.VMEM)
SM = pl.BlockSpec(memory_space=pltpu.SMEM)
ANY = pl.BlockSpec(memory_space=pl.ANY)
HBM = pl.BlockSpec(memory_space=pltpu.HBM)


def dot(a, b):
    return jnp.dot(a, b, preferred_element_type=F32)


def params(mib):
    return pltpu.CompilerParams(vmem_limit_bytes=mib << 20)


def cost(flops, moved):
    return pl.CostEstimate(flops=flops, bytes_accessed=moved, transcendentals=0)


def moves(dx, dz):
    return [
        (z * SIDE + x, (z + dz) % SIDE * SIDE + (x + dx) % SIDE)
        for z in range(SIDE)
        for x in range(SIDE)
    ]


def eye():
    return lax.broadcasted_iota(I32, (128, 128), 0) == lax.broadcasted_iota(I32, (128, 128), 1)


def to_row(column):
    return jnp.sum(jnp.where(eye(), column, 0.0), axis=0, keepdims=True)


def to_column(row):
    return jnp.sum(jnp.where(eye(), row, 0.0), axis=1, keepdims=True)


def split3(value):
    top = value.astype(BF16)
    rest = value - top.astype(F32)
    mid = rest.astype(BF16)
    return top, mid, (rest - mid.astype(F32)).astype(BF16)


def work_table():
    table = np.zeros((SIDE * SIDE, 2, TILES + 1), np.int32)
    for z in range(SIDE):
        for x in range(SIDE):
            tiles = []
            for d in range(SIDE):
                for e in range(SIDE):
                    late = (d == 2) + (e == 2)
                    first_z = (z + e) % SIDE
                    if first_z < z or (e == 0 and x < (x + d) % SIDE):
                        tiles.append((late, d, 3 + e if e else 0))
                    second_z = (z + d) % SIDE
                    if second_z > z or (d == 0 and (x + e) % SIDE < x):
                        tiles.append((late, 4 + d, e))
            assert len(tiles) == TILES
            for n, (_, q, k) in enumerate(sorted(tiles)):
                table[z * SIDE + x, :, n] = q, k
    return table


def start_copies(x_hbm, weights, x, w, sems):
    copies = []
    for n, source in enumerate(weights):
        dest = w.at[:, pl.ds(128 * n, 128)]
        copies.append(pltpu.make_async_copy(source, dest, sems.at[4 + n]))
    for i in range(4):
        rows = pl.ds(256 * i, 256)
        copies.append(pltpu.make_async_copy(x_hbm.at[rows], x.at[rows], sems.at[i]))
    for c in copies:
        c.start()
    for c in copies[:-4]:
        c.wait()
    return copies[-4:]


def project_kernel(x_hbm, wq, wk, wv, gate, px, pz, x, w, sems):
    arrivals = start_copies(x_hbm, (wk, wv, wq), x, w, sems)
    zero = jnp.zeros((8, 128), BF16)
    top, mid, low = split3(gate[...] * (-LOG2E))
    gates = jnp.concatenate(
        [jnp.concatenate([top, mid], axis=1), jnp.concatenate([low, zero], axis=1)], axis=0
    )
    px[GATE_ROW : GATE_ROW + 16, :] = gates
    pz[GATE_ROW : GATE_ROW + 16, :] = gates
    for i in range(4):
        arrivals[i].wait()
        out = dot(x[256 * i : 256 * i + 256, :], w[...]).astype(BF16)
        px[256 * i : 256 * i + 256, :] = out[:, :256]
        pz[256 * i : 256 * i + 256, :] = out[:, :256]
        dest = px if i < 2 else pz
        lane = 128 * (i % 2)
        dest[QUERY_ROW:PACK_ROWS, lane : lane + 128] = out[:, 256:]


def project(x, wq, wk, wv, gate):
    pack = jax.ShapeDtypeStruct((PACK_ROWS, 256), BF16)
    return pl.pallas_call(
        project_kernel,
        out_shape=(pack, pack),
        in_specs=[HBM, HBM, HBM, HBM, VM],
        out_specs=(VM, VM),
        scratch_shapes=[
            pltpu.VMEM((TOK, 2048), BF16),
            pltpu.VMEM((2048, 384), BF16),
            pltpu.SemaphoreType.DMA((7,)),
        ],
        compiler_params=params(12),
        cost_estimate=cost(2 * TOK * 2048 * 512, 8 << 20),
        name="project",
    )(x, wq, wk, wv, gate)


def glu_kernel(x_hbm, wu, wg, after, out, x, w, sems):
    arrivals = start_copies(x_hbm, (wu, wg), x, w, sems)
    for i in range(4):
        arrivals[i].wait()
        both = dot(x[256 * i : 256 * i + 256, :], w[...])
        out[256 * i : 256 * i + 256, :] = (both[:, :128] * jax.nn.sigmoid(both[:, 128:])).astype(
            BF16
        )


def glu(x, wu, wg, after):
    return pl.pallas_call(
        glu_kernel,
        out_shape=jax.ShapeDtypeStruct((TOK, 128), BF16),
        in_specs=[HBM, HBM, HBM, ANY],
        out_specs=VM,
        scratch_shapes=[
            pltpu.VMEM((TOK, 2048), BF16),
            pltpu.VMEM((2048, 256), BF16),
            pltpu.SemaphoreType.DMA((6,)),
        ],
        compiler_params=params(10),
        cost_estimate=cost(2 * TOK * 2048 * 256, 6 << 20),
        name="glu",
    )(x, wu, wg, after)


def conv_kernel(gated, halo, taps, gain, out, padded):
    padded[0:32, :] = halo[...].astype(F32)
    padded[32 : 32 + TOK, :] = gated[...].astype(F32)
    padded[32 + TOK :, :] = jnp.zeros((8, 128), F32)
    for block in range(8):
        start = 128 * block
        total = None
        for r in range(8):
            part = None
            for q in range(5):
                j = 8 * q + r - 2
                if 0 <= j < TAPS:
                    term = taps[j : j + 1, :] * padded[start + 8 * q : start + 8 * q + 136, :]
                    part = term if part is None else part + term
            part = part[r : r + 128, :]
            total = part if total is None else total + part
        out[block, 0:128, :] = total
        out[block, 128:136, :] = jnp.broadcast_to(gain[...], (8, 128))


def convolve(gated, halo, taps, gain):
    return pl.pallas_call(
        conv_kernel,
        out_shape=jax.ShapeDtypeStruct((8, 136, 128), F32),
        in_specs=[VM] * 4,
        out_specs=VM,
        scratch_shapes=[pltpu.VMEM((TOK + 40, 128), F32)],
        compiler_params=params(8),
        cost_estimate=cost(2 * TOK * 128 * 31 * 64, 1 << 20),
        name="convolve",
    )(gated, halo, taps, gain)


def diagonal_kernel(px, pz, after, m_out, l_out, acc_out):
    top = px[GATE_ROW : GATE_ROW + 8, :].astype(F32)
    low = px[GATE_ROW + 8 : GATE_ROW + 16, :].astype(F32)
    gates = top[:, :128] + top[:, 128:] + low[:, :128]
    for half, pack in ((0, px), (1, pz)):
        keys = HALF * (half + 1)
        query = jnp.concatenate(
            [pack[QUERY_ROW:PACK_ROWS, :128], pack[QUERY_ROW:PACK_ROWS, 128:]], axis=0
        )
        scores = lax.dot_general(
            query, px[:keys, :128], (((1,), (1,)), ((), ())), preferred_element_type=F32
        )
        row = lax.broadcasted_iota(I32, (HALF, 128), 0) + HALF * half
        lane = lax.broadcasted_iota(I32, (HALF, 128), 1)
        parts = []
        for c in range(keys // 128):
            t = scores[:, 128 * c : 128 * c + 128] * SCALE + gates[c : c + 1, :]
            parts.append(jnp.where(lane + 128 * c <= row, t, LOW))
        most = functools.reduce(jnp.maximum, parts)
        most = jnp.broadcast_to(jnp.max(most, axis=1, keepdims=True), (HALF, 128))
        weights = [jnp.exp2(t - most) for t in parts]
        m_out[half] = most
        l_out[half] = functools.reduce(jnp.add, weights)
        acc_out[half] = dot(
            jnp.concatenate([w.astype(BF16) for w in weights], axis=1), px[:keys, 128:]
        )


def diagonal(px, pz, after):
    state = jax.ShapeDtypeStruct((2, HALF, 128), F32)
    return pl.pallas_call(
        diagonal_kernel,
        out_shape=(state, state, state),
        in_specs=[VM, VM, ANY],
        out_specs=(VM, VM, VM),
        compiler_params=params(16),
        cost_estimate=cost(2 * HALF * 2048 * 512, 4 << 20),
        name="diagonal",
    )(px, pz, after)


def attend_kernel(
    table, own, px, x1, x2, x3, pz, z1, z2, z3, m_in, l_in, acc_in,
    o_own, lse_own, a1, a2, a3, b1, b2, b3,
    packs, query, gates, sa, sb, ma, mb, aa, ab, m, l, acc, sems,
):
    sources = (px, x1, x2, x3, z1, z2, z3)
    copies = [
        pltpu.make_async_copy(source, packs.at[n], sems.at[n]) for n, source in enumerate(sources)
    ]
    copies.append(pltpu.make_async_copy(pz, packs.at[7], sems.at[7]))
    for c in copies:
        c.start()
    m[...] = jnp.full_like(m, LOW)
    l[...] = jnp.zeros_like(l)
    acc[...] = jnp.zeros_like(acc)
    for half in range(2):
        m[4 * half] = m_in[half]
        l[4 * half] = l_in[half]
        acc[4 * half] = acc_in[half]
    for c in copies:
        c.wait()
    for n, slot in enumerate((0, 1, 2, 3, 7, 4, 5, 6)):
        for side in range(2):
            query[n, 256 * side : 256 * side + 256, :] = packs[
                slot, QUERY_ROW:PACK_ROWS, 128 * side : 128 * side + 128
            ]
    for n in range(7):
        top = packs[n, GATE_ROW : GATE_ROW + 8, :].astype(F32)
        low = packs[n, GATE_ROW + 8 : GATE_ROW + 16, :].astype(F32)
        gates[n] = top[:, :128] + top[:, 128:] + low[:, :128]
    row = own[0]

    def scores_of(n, s, most, shrink):
        q, k = table[row, 0, n], table[row, 1, n]
        raw = lax.dot_general(
            query[q], packs[k, :TOK, :128], (((1,), (1,)), ((), ())), preferred_element_type=F32
        )
        best = None
        for c in range(8):
            t = raw[:, 128 * c : 128 * c + 128] * SCALE + gates[k, c : c + 1, :]
            s[:, 128 * c : 128 * c + 128] = t
            best = t if best is None else jnp.maximum(best, t)
        old = m[q]
        new = jnp.maximum(old, jnp.max(best, axis=1, keepdims=True))
        shrink[...] = jnp.exp2(old - new)
        m[q] = new
        most[...] = new

    def weigh(n, s, most, shrink):
        q, k = table[row, 0, n], table[row, 1, n]
        top = most[...]
        by = shrink[...]
        w = [jnp.exp2(s[:, 128 * c : 128 * c + 128] - top) for c in range(8)]
        total = ((w[0] + w[1]) + (w[2] + w[3])) + ((w[4] + w[5]) + (w[6] + w[7]))
        rounded = jnp.concatenate([v.astype(BF16) for v in w], axis=1)
        l[q] = l[q] * by + total
        acc[q] = acc[q] * by + dot(rounded, packs[k, :TOK, 128:])

    first, second = (sa, ma, aa), (sb, mb, ab)
    scores_of(0, *first)

    def two_tiles(i, carry):
        scores_of(2 * i + 1, *second)
        weigh(2 * i, *first)
        scores_of(2 * i + 2, *first)
        weigh(2 * i + 1, *second)
        return carry

    lax.fori_loop(0, (TILES - 1) // 2, two_tiles, 0)
    weigh(TILES - 1, *first)
    for n, out in enumerate((None, a1, a2, a3, None, b1, b2, b3)):
        total = jnp.maximum(jnp.sum(l[n], axis=1, keepdims=True), TINY)
        mixed = acc[n] / total
        lse = m[n] + jnp.log2(total)
        if out is None:
            o_own[n // 4] = mixed
            lse_own[n // 4] = lse
        else:
            out[0:HALF, :] = mixed.astype(BF16)
            rows = [to_row(lse[128 * b : 128 * b + 128, :]) for b in range(4)]
            parts = split3(jnp.concatenate(rows + rows, axis=0))
            out[HALF : HALF + 16, :] = jnp.concatenate(
                [parts[0][:4], parts[1][:4], parts[2]], axis=0
            )


def attend(table, own, packs, state):
    back = jax.ShapeDtypeStruct((BACK_ROWS, 128), BF16)
    kept = jax.ShapeDtypeStruct((2, HALF, 128), F32)
    per_tile = [pltpu.VMEM((HALF, 128), F32)] * 4
    return pl.pallas_call(
        attend_kernel,
        out_shape=(kept, kept) + (back,) * 6,
        in_specs=[SM, SM] + [ANY] * 8 + [VM] * 3,
        out_specs=(VM,) * 8,
        scratch_shapes=[
            pltpu.VMEM((8, PACK_ROWS, 256), BF16),
            pltpu.VMEM((8, HALF, 128), BF16),
            pltpu.VMEM((7, 8, 128), F32),
            pltpu.VMEM((HALF, TOK), F32),
            pltpu.VMEM((HALF, TOK), F32),
            *per_tile,
            *[pltpu.VMEM((8, HALF, 128), F32)] * 3,
            pltpu.SemaphoreType.DMA((8,)),
        ],
        compiler_params=params(28),
        cost_estimate=cost(TILES * 4 * HALF * TOK * 256, 8 << 20),
        name="attend",
    )(table, own, *packs, *state)


def combine_kernel(o_own, lse_own, a1, a2, a3, b1, b2, b3, out):
    for half, backs in ((0, (a1, a2, a3)), (1, (b1, b2, b3))):
        lses = []
        for back in backs:
            tail = back[HALF : HALF + 16, :].astype(F32)
            lses.append(tail[0:4] + tail[4:8] + tail[8:12])
        for b in range(4):
            rows = slice(128 * b, 128 * b + 128)
            columns = [lse_own[half, rows, :]]
            columns += [jnp.broadcast_to(to_column(v[b : b + 1, :]), (128, 128)) for v in lses]
            most = functools.reduce(jnp.maximum, columns)
            shares = [jnp.exp2(c - most) for c in columns]
            mixed = shares[0] * o_own[half, rows, :]
            for share, back in zip(shares[1:], backs):
                mixed = mixed + share * back[rows, :].astype(F32)
            out[4 * half + b] = (mixed / functools.reduce(jnp.add, shares)).astype(BF16)


def combine(o_own, lse_own, backs):
    return pl.pallas_call(
        combine_kernel,
        out_shape=jax.ShapeDtypeStruct((8, 128, 128), BF16),
        in_specs=[VM] * 8,
        out_specs=VM,
        compiler_params=params(16),
        cost_estimate=cost(1 << 29, 2 << 20),
        name="combine",
    )(o_own, lse_own, *backs)


def conv_out_kernel(parts, w_hbm, out, later, rows, w, sems):
    copies = []
    for j in range(4):
        cols = pl.ds(512 * j, 512)
        copies.append(
            pltpu.make_async_copy(w_hbm.at[pl.ds(0, 1024), cols], w.at[:, cols], sems.at[j])
        )
    copies.append(pltpu.make_async_copy(w_hbm.at[pl.ds(1024, 1024)], later, sems.at[4]))
    for c in copies:
        c.start()
    total = functools.reduce(jnp.add, [parts[c, :128, :] for c in range(8)])
    mean = jnp.sum(total, axis=1, keepdims=True) * (1.0 / 1024)
    far = [parts[c, :128, :] - mean for c in range(8)]
    spread = functools.reduce(jnp.add, [v * v for v in far])
    spread = jnp.sum(spread, axis=1, keepdims=True) * (1.0 / 1024)
    inverse = lax.rsqrt(spread + EPS)
    for c in range(8):
        v = far[c] * inverse * parts[c, 128:129, :]
        rows[:, 128 * c : 128 * c + 128] = (v * jax.nn.sigmoid(v)).astype(BF16)
    for j in range(4):
        copies[j].wait()
        out[:, 512 * j : 512 * j + 512] = dot(rows[...], w[:, 512 * j : 512 * j + 512])
    copies[4].wait()


def conv_out(parts, w):
    return pl.pallas_call(
        conv_out_kernel,
        out_shape=(
            jax.ShapeDtypeStruct((128, 2048), F32),
            jax.ShapeDtypeStruct((1024, 2048), BF16),
        ),
        in_specs=[VM, HBM],
        out_specs=(VM, VM),
        scratch_shapes=[
            pltpu.VMEM((128, 1024), BF16),
            pltpu.VMEM((1024, 2048), BF16),
            pltpu.SemaphoreType.DMA((5,)),
        ],
        compiler_params=params(14),
        cost_estimate=cost(2 * 128 * 1024 * 2048 * 4, 6 << 20),
        name="conv_out",
    )(parts, w)


def attn_out_kernel(parts, conv, w, out, rows):
    for c in range(8):
        rows[:, 128 * c : 128 * c + 128] = parts[c]
    for j in range(4):
        cols = slice(512 * j, 512 * j + 512)
        out[:, cols] = (dot(rows[...], w[:, cols]) + conv[:, cols]).astype(BF16)


def attn_out(parts, conv, w):
    return pl.pallas_call(
        attn_out_kernel,
        out_shape=jax.ShapeDtypeStruct((128, 2048), BF16),
        in_specs=[VM, VM, VM],
        out_specs=VM,
        scratch_shapes=[pltpu.VMEM((128, 1024), BF16)],
        compiler_params=params(10),
        cost_estimate=cost(2 * 128 * 1024 * 2048 * 4, 6 << 20),
        name="attn_out",
    )(parts, conv, w)


def layer(x, wq, wk, wv, wu, wg, taps, gain, gate, w_out):
    x, wq, wk, wv, wu, wg, w_out = (
        pltpu.with_memory_space_constraint(v, pltpu.HBM) for v in (x, wq, wk, wv, wu, wg, w_out)
    )
    own = lax.axis_index("sp").astype(I32).reshape(1)
    table = jnp.asarray(work_table())
    px, pz = project(x, wq, wk, wv, gate.reshape(8, 128))
    xs, zs = [None] * 4, [None] * 4
    for d in (1, 3, 2):
        xs[d] = lax.ppermute(px, "sp", moves(-d, 0))
        zs[d] = lax.ppermute(pz, "sp", moves(0, -d))
    gated = glu(x, wu, wg, px)
    halo = lax.ppermute(gated[TOK - 32 :], "sp", [(i, i + 1) for i in range(15)])
    conv = convolve(gated, halo, taps, gain.reshape(1, 128))
    conv_parts = lax.all_to_all(conv, "tp", 0, 0, tiled=True)
    conv_mixed, w_attn = conv_out(conv_parts, w_out)
    state = diagonal(px, pz, conv_mixed)
    packs = (px, *xs[1:], pz, *zs[1:])
    o_own, lse_own, *sent = attend(table, own, packs, state)
    backs = [lax.ppermute(sent[d - 1], "sp", moves(d, 0)) for d in (1, 2, 3)]
    backs += [lax.ppermute(sent[d + 2], "sp", moves(0, d)) for d in (1, 2, 3)]
    mixed = combine(o_own, lse_own, backs)
    attn_parts = lax.all_to_all(mixed, "tp", 0, 0, tiled=True)
    return attn_out(attn_parts, conv_mixed, w_attn)


def solution(mesh):
    in_specs = (
        P("sp", None),
        P(None, "tp"),
        P(None, "tp"),
        P(None, "tp"),
        P(None, "tp"),
        P(None, "tp"),
        P(None, "tp"),
        P("tp"),
        P("sp", "tp"),
        P(),
    )
    out_specs = P(("sp", "tp"), None)
    return jax.shard_map(layer, mesh=mesh, in_specs=in_specs, out_specs=out_specs, check_vma=False)
```

```python
import functools

import jax
import jax.numpy as jnp
import numpy as np
from jax import lax
from jax.experimental import pallas as pl
from jax.experimental.pallas import tpu as pltpu
from jax.sharding import PartitionSpec as P


BF16, F32, I32 = jnp.bfloat16, jnp.float32, jnp.int32
SIDE = 4
HEAD = 128
TOK = 1024
HALF = 512
TAPS = 31
GATE_ROW = TOK
QUERY_ROW = TOK + 16
PACK_ROWS = QUERY_ROW + HALF // 2
BACK_ROWS = HALF + 16
TILES = 15
LOG2E = 1.4426950408889634
SCALE = HEAD**-0.5 * LOG2E
LOW = -1e30
TINY = 1e-37
EPS = 1e-05

VM = pl.BlockSpec(memory_space=pltpu.VMEM)
SM = pl.BlockSpec(memory_space=pltpu.SMEM)
ANY = pl.BlockSpec(memory_space=pl.ANY)
HBM = pl.BlockSpec(memory_space=pltpu.HBM)


def dot(a, b):
    return jnp.dot(a, b, preferred_element_type=F32)


def params(mib):
    return pltpu.CompilerParams(vmem_limit_bytes=mib << 20)


def cost(flops, moved):
    return pl.CostEstimate(flops=flops, bytes_accessed=moved, transcendentals=0)


def moves(dx, dz):
    return [
        (z * SIDE + x, (z + dz) % SIDE * SIDE + (x + dx) % SIDE)
        for z in range(SIDE)
        for x in range(SIDE)
    ]


def eye():
    return lax.broadcasted_iota(I32, (128, 128), 0) == lax.broadcasted_iota(I32, (128, 128), 1)


def to_row(column):
    return jnp.sum(jnp.where(eye(), column, 0.0), axis=0, keepdims=True)


def to_column(row):
    return jnp.sum(jnp.where(eye(), row, 0.0), axis=1, keepdims=True)


def split3(value):
    top = value.astype(BF16)
    rest = value - top.astype(F32)
    mid = rest.astype(BF16)
    return top, mid, (rest - mid.astype(F32)).astype(BF16)


def work_table():
    table = np.zeros((SIDE * SIDE, 2, TILES + 1), np.int32)
    for z in range(SIDE):
        for x in range(SIDE):
            tiles = []
            for d in range(SIDE):
                for e in range(SIDE):
                    late = d == 2 or e == 2
                    first_z = (z + e) % SIDE
                    if first_z < z or (e == 0 and x < (x + d) % SIDE):
                        tiles.append((late, d, 4 + e if e else 0))
                    second_z = (z + d) % SIDE
                    if second_z > z or (d == 0 and (x + e) % SIDE < x):
                        tiles.append((late, 4 + d, e))
            assert len(tiles) == TILES and sum(not t[0] for t in tiles) == 8
            for n, (_, q, k) in enumerate(sorted(tiles)):
                table[z * SIDE + x, :, n] = q, k
    return table


def start_copies(x_hbm, weights, x, w, sems):
    copies = []
    for n, source in enumerate(weights):
        dest = w.at[:, pl.ds(128 * n, 128)]
        copies.append(pltpu.make_async_copy(source, dest, sems.at[4 + n]))
    for i in range(4):
        rows = pl.ds(256 * i, 256)
        copies.append(pltpu.make_async_copy(x_hbm.at[rows], x.at[rows], sems.at[i]))
    for c in copies:
        c.start()
    for c in copies[:-4]:
        c.wait()
    return copies[-4:]


def gate_rows(both):
    return (both[:, :128] * jax.nn.sigmoid(both[:, 128:])).astype(BF16)


def project_kernel(x_hbm, wq, wk, wv, wu, wg, gate, px, pz, tail, x, w, sems):
    arrivals = start_copies(x_hbm, (wk, wv, wq, wu, wg), x, w, sems)
    zero = jnp.zeros((8, 128), BF16)
    top, mid, low = split3(gate[...] * (-LOG2E))
    gates = jnp.concatenate(
        [jnp.concatenate([top, mid], axis=1), jnp.concatenate([low, zero], axis=1)], axis=0
    )
    px[GATE_ROW : GATE_ROW + 16, :] = gates
    pz[GATE_ROW : GATE_ROW + 16, :] = gates
    for i in range(4):
        arrivals[i].wait()
        out = dot(x[256 * i : 256 * i + 256, :], w[:, :384]).astype(BF16)
        px[256 * i : 256 * i + 256, :] = out[:, :256]
        pz[256 * i : 256 * i + 256, :] = out[:, :256]
        dest = px if i < 2 else pz
        lane = 128 * (i % 2)
        dest[QUERY_ROW:PACK_ROWS, lane : lane + 128] = out[:, 256:]
    tail[...] = gate_rows(dot(x[TOK - 32 :, :], w[:, 384:]))


def project(x, wq, wk, wv, wu, wg, gate):
    pack = jax.ShapeDtypeStruct((PACK_ROWS, 256), BF16)
    return pl.pallas_call(
        project_kernel,
        out_shape=(pack, pack, jax.ShapeDtypeStruct((32, 128), BF16)),
        in_specs=[HBM] * 6 + [VM],
        out_specs=(VM, VM, VM),
        scratch_shapes=[
            pltpu.VMEM((TOK, 2048), BF16),
            pltpu.VMEM((2048, 640), BF16),
            pltpu.SemaphoreType.DMA((9,)),
        ],
        compiler_params=params(12),
        cost_estimate=cost(2 * TOK * 2048 * 512, 8 << 20),
        name="project",
    )(x, wq, wk, wv, wu, wg, gate)


def glu_kernel(x_hbm, wu, wg, after, out, x, w, sems):
    arrivals = start_copies(x_hbm, (wu, wg), x, w, sems)
    for i in range(4):
        arrivals[i].wait()
        out[256 * i : 256 * i + 256, :] = gate_rows(dot(x[256 * i : 256 * i + 256, :], w[...]))


def glu(x, wu, wg, after):
    return pl.pallas_call(
        glu_kernel,
        out_shape=jax.ShapeDtypeStruct((TOK, 128), BF16),
        in_specs=[HBM, HBM, HBM, ANY],
        out_specs=VM,
        scratch_shapes=[
            pltpu.VMEM((TOK, 2048), BF16),
            pltpu.VMEM((2048, 256), BF16),
            pltpu.SemaphoreType.DMA((6,)),
        ],
        compiler_params=params(10),
        cost_estimate=cost(2 * TOK * 2048 * 256, 6 << 20),
        name="glu",
    )(x, wu, wg, after)


def conv_kernel(gated, halo, taps, gain, out, padded):
    padded[0:32, :] = halo[...].astype(F32)
    padded[32 : 32 + TOK, :] = gated[...].astype(F32)
    padded[32 + TOK :, :] = jnp.zeros((8, 128), F32)
    for block in range(8):
        start = 128 * block
        total = None
        for r in range(8):
            part = None
            for q in range(5):
                j = 8 * q + r - 2
                if 0 <= j < TAPS:
                    term = taps[j : j + 1, :] * padded[start + 8 * q : start + 8 * q + 136, :]
                    part = term if part is None else part + term
            part = part[r : r + 128, :]
            total = part if total is None else total + part
        out[block, 0:128, :] = total
        out[block, 128:136, :] = jnp.broadcast_to(gain[...], (8, 128))


def convolve(gated, halo, taps, gain):
    return pl.pallas_call(
        conv_kernel,
        out_shape=jax.ShapeDtypeStruct((8, 136, 128), F32),
        in_specs=[VM] * 4,
        out_specs=VM,
        scratch_shapes=[pltpu.VMEM((TOK + 40, 128), F32)],
        compiler_params=params(8),
        cost_estimate=cost(2 * TOK * 128 * 31 * 64, 1 << 20),
        name="convolve",
    )(gated, halo, taps, gain)


def diagonal_kernel(px, pz, m_out, l_out, acc_out):
    top = px[GATE_ROW : GATE_ROW + 8, :].astype(F32)
    low = px[GATE_ROW + 8 : GATE_ROW + 16, :].astype(F32)
    gates = top[:, :128] + top[:, 128:] + low[:, :128]
    for half, pack in ((0, px), (1, pz)):
        keys = HALF * (half + 1)
        query = jnp.concatenate(
            [pack[QUERY_ROW:PACK_ROWS, :128], pack[QUERY_ROW:PACK_ROWS, 128:]], axis=0
        )
        scores = lax.dot_general(
            query, px[:keys, :128], (((1,), (1,)), ((), ())), preferred_element_type=F32
        )
        row = lax.broadcasted_iota(I32, (HALF, 128), 0) + HALF * half
        lane = lax.broadcasted_iota(I32, (HALF, 128), 1)
        parts = []
        for c in range(keys // 128):
            t = scores[:, 128 * c : 128 * c + 128] * SCALE + gates[c : c + 1, :]
            parts.append(jnp.where(lane + 128 * c <= row, t, LOW))
        most = functools.reduce(jnp.maximum, parts)
        most = jnp.broadcast_to(jnp.max(most, axis=1, keepdims=True), (HALF, 128))
        weights = [jnp.exp2(t - most) for t in parts]
        m_out[half] = most
        l_out[half] = functools.reduce(jnp.add, weights)
        acc_out[half] = dot(
            jnp.concatenate([w.astype(BF16) for w in weights], axis=1), px[:keys, 128:]
        )


def diagonal(px, pz):
    state = jax.ShapeDtypeStruct((2, HALF, 128), F32)
    return pl.pallas_call(
        diagonal_kernel,
        out_shape=(state, state, state),
        in_specs=[VM, VM],
        out_specs=(VM, VM, VM),
        compiler_params=params(16),
        cost_estimate=cost(2 * HALF * 2048 * 512, 4 << 20),
        name="diagonal",
    )(px, pz)


PACKS = 8
NEAR, FAR = 8, 7


def load_packs(sources, packs, query, gates, sems):
    copies = [pltpu.make_async_copy(src, packs.at[n], sems.at[n]) for n, src in sources]
    for c in copies:
        c.start()
    for c in copies:
        c.wait()
    for slot, _ in sources:
        for side in range(2):
            query[slot, 256 * side : 256 * side + 256, :] = packs[
                slot, QUERY_ROW:PACK_ROWS, 128 * side : 128 * side + 128
            ]
        top = packs[slot, GATE_ROW : GATE_ROW + 8, :].astype(F32)
        low = packs[slot, GATE_ROW + 8 : GATE_ROW + 16, :].astype(F32)
        gates[slot] = top[:, :128] + top[:, 128:] + low[:, :128]


def run_tiles(table, own, start, count, packs, query, gates, per_tile, m, l, acc):
    sa, sb, ma, mb, aa, ab = per_tile
    row = own[0]
    first, second = (sa, ma, aa), (sb, mb, ab)

    def scores_of(n, s, most, shrink):
        q, k = table[row, 0, n], table[row, 1, n]
        raw = lax.dot_general(
            query[q], packs[k, :TOK, :128], (((1,), (1,)), ((), ())), preferred_element_type=F32
        )
        best = None
        for c in range(8):
            t = raw[:, 128 * c : 128 * c + 128] * SCALE + gates[k, c : c + 1, :]
            s[:, 128 * c : 128 * c + 128] = t
            best = t if best is None else jnp.maximum(best, t)
        old = m[q]
        new = jnp.maximum(old, jnp.max(best, axis=1, keepdims=True))
        shrink[...] = jnp.exp2(old - new)
        m[q] = new
        most[...] = new

    def weigh(n, s, most, shrink):
        q, k = table[row, 0, n], table[row, 1, n]
        top = most[...]
        by = shrink[...]
        w = [jnp.exp2(s[:, 128 * c : 128 * c + 128] - top) for c in range(8)]
        total = ((w[0] + w[1]) + (w[2] + w[3])) + ((w[4] + w[5]) + (w[6] + w[7]))
        rounded = jnp.concatenate([v.astype(BF16) for v in w], axis=1)
        l[q] = l[q] * by + total
        acc[q] = acc[q] * by + dot(rounded, packs[k, :TOK, 128:])


    scores_of(start, *first)

    def two_tiles(i, carry):
        n = start + 2 * i
        scores_of(n + 1, *second)
        weigh(n, *first)
        scores_of(n + 2, *first)
        weigh(n + 1, *second)
        return carry

    lax.fori_loop(0, (count - 1) // 2, two_tiles, 0)
    if count % 2 == 0:
        scores_of(start + count - 1, *second)
        weigh(start + count - 2, *first)
        weigh(start + count - 1, *second)
    else:
        weigh(start + count - 1, *first)


def near_kernel(
    table, own, px, x1, x3, pz, z1, z3, m_in, l_in, acc_in, after, m, l, acc,
    packs, query, gates, sems, *per_tile,
):
    sources = ((0, px), (1, x1), (3, x3), (4, pz), (5, z1), (7, z3))
    for half in range(2):
        m[4 * half] = m_in[half]
        l[4 * half] = l_in[half]
        acc[4 * half] = acc_in[half]
    for n in (1, 3, 5, 7):
        m[n] = jnp.full((HALF, 128), LOW, F32)
        l[n] = jnp.zeros((HALF, 128), F32)
        acc[n] = jnp.zeros((HALF, 128), F32)
    load_packs(sources, packs, query, gates, sems)
    run_tiles(table, own, 0, NEAR, packs, query, gates, per_tile, m, l, acc)


def far_kernel(
    table, own, px, x1, x2, x3, pz, z1, z2, z3, m_in, l_in, acc_in,
    o_own, lse_own, a1, a2, a3, b1, b2, b3,
    packs, query, gates, sems, m, l, acc, *per_tile,
):
    sources = ((0, px), (1, x1), (2, x2), (3, x3), (4, pz), (5, z1), (6, z2), (7, z3))
    for n in (0, 1, 3, 4, 5, 7):
        m[n] = m_in[n]
        l[n] = l_in[n]
        acc[n] = acc_in[n]
    for n in (2, 6):
        m[n] = jnp.full((HALF, 128), LOW, F32)
        l[n] = jnp.zeros((HALF, 128), F32)
        acc[n] = jnp.zeros((HALF, 128), F32)
    load_packs(sources, packs, query, gates, sems)
    run_tiles(table, own, NEAR, FAR, packs, query, gates, per_tile, m, l, acc)
    for n, out in enumerate((None, a1, a2, a3, None, b1, b2, b3)):
        total = jnp.maximum(jnp.sum(l[n], axis=1, keepdims=True), TINY)
        mixed = acc[n] / total
        lse = m[n] + jnp.log2(total)
        if out is None:
            o_own[n // 4] = mixed
            lse_own[n // 4] = lse
        else:
            out[0:HALF, :] = mixed.astype(BF16)
            rows = [to_row(lse[128 * b : 128 * b + 128, :]) for b in range(4)]
            parts = split3(jnp.concatenate(rows + rows, axis=0))
            out[HALF : HALF + 16, :] = jnp.concatenate(
                [parts[0][:4], parts[1][:4], parts[2]], axis=0
            )


SLOT_SCRATCH = [
    pltpu.VMEM((PACKS, PACK_ROWS, 256), BF16),
    pltpu.VMEM((PACKS, HALF, 128), BF16),
    pltpu.VMEM((PACKS, 8, 128), F32),
    pltpu.SemaphoreType.DMA((PACKS,)),
]
TILE_SCRATCH = [pltpu.VMEM((HALF, TOK), F32)] * 2 + [pltpu.VMEM((HALF, 128), F32)] * 4
STATE_SCRATCH = [pltpu.VMEM((PACKS, HALF, 128), F32)] * 3


def attend_near(table, own, packs, state, after):
    kept = jax.ShapeDtypeStruct((PACKS, HALF, 128), F32)
    return pl.pallas_call(
        near_kernel,
        out_shape=(kept, kept, kept),
        in_specs=[SM, SM] + [ANY] * 6 + [VM] * 3 + [ANY],
        out_specs=(VM,) * 3,
        scratch_shapes=SLOT_SCRATCH + TILE_SCRATCH,
        compiler_params=params(24),
        cost_estimate=cost(NEAR * 4 * HALF * TOK * 256, 8 << 20),
        name="attend_near",
    )(table, own, *packs, *state, after)


def attend_far(table, own, packs, state):
    back = jax.ShapeDtypeStruct((BACK_ROWS, 128), BF16)
    kept = jax.ShapeDtypeStruct((2, HALF, 128), F32)
    return pl.pallas_call(
        far_kernel,
        out_shape=(kept, kept) + (back,) * 6,
        in_specs=[SM, SM] + [ANY] * 8 + [VM] * 3,
        out_specs=(VM,) * 8,
        scratch_shapes=SLOT_SCRATCH + STATE_SCRATCH + TILE_SCRATCH,
        compiler_params=params(30),
        cost_estimate=cost(FAR * 4 * HALF * TOK * 256, 8 << 20),
        name="attend_far",
    )(table, own, *packs, *state)


def combine_kernel(o_own, lse_own, a1, a2, a3, b1, b2, b3, out):
    for half, backs in ((0, (a1, a2, a3)), (1, (b1, b2, b3))):
        lses = []
        for back in backs:
            tail = back[HALF : HALF + 16, :].astype(F32)
            lses.append(tail[0:4] + tail[4:8] + tail[8:12])
        for b in range(4):
            rows = slice(128 * b, 128 * b + 128)
            columns = [lse_own[half, rows, :]]
            columns += [jnp.broadcast_to(to_column(v[b : b + 1, :]), (128, 128)) for v in lses]
            most = functools.reduce(jnp.maximum, columns)
            shares = [jnp.exp2(c - most) for c in columns]
            mixed = shares[0] * o_own[half, rows, :]
            for share, back in zip(shares[1:], backs):
                mixed = mixed + share * back[rows, :].astype(F32)
            out[4 * half + b] = (mixed / functools.reduce(jnp.add, shares)).astype(BF16)


def combine(o_own, lse_own, backs):
    return pl.pallas_call(
        combine_kernel,
        out_shape=jax.ShapeDtypeStruct((8, 128, 128), BF16),
        in_specs=[VM] * 8,
        out_specs=VM,
        compiler_params=params(16),
        cost_estimate=cost(1 << 29, 2 << 20),
        name="combine",
    )(o_own, lse_own, *backs)


def conv_out_kernel(parts, w_hbm, out, later, rows, w, sems):
    copies = []
    for j in range(4):
        cols = pl.ds(512 * j, 512)
        copies.append(
            pltpu.make_async_copy(w_hbm.at[pl.ds(0, 1024), cols], w.at[:, cols], sems.at[j])
        )
    copies.append(pltpu.make_async_copy(w_hbm.at[pl.ds(1024, 1024)], later, sems.at[4]))
    for c in copies:
        c.start()
    total = functools.reduce(jnp.add, [parts[c, :128, :] for c in range(8)])
    mean = jnp.sum(total, axis=1, keepdims=True) * (1.0 / 1024)
    far = [parts[c, :128, :] - mean for c in range(8)]
    spread = functools.reduce(jnp.add, [v * v for v in far])
    spread = jnp.sum(spread, axis=1, keepdims=True) * (1.0 / 1024)
    inverse = lax.rsqrt(spread + EPS)
    for c in range(8):
        v = far[c] * inverse * parts[c, 128:129, :]
        rows[:, 128 * c : 128 * c + 128] = (v * jax.nn.sigmoid(v)).astype(BF16)
    for j in range(4):
        copies[j].wait()
        out[:, 512 * j : 512 * j + 512] = dot(rows[...], w[:, 512 * j : 512 * j + 512])
    copies[4].wait()


def conv_out(parts, w):
    return pl.pallas_call(
        conv_out_kernel,
        out_shape=(
            jax.ShapeDtypeStruct((128, 2048), F32),
            jax.ShapeDtypeStruct((1024, 2048), BF16),
        ),
        in_specs=[VM, HBM],
        out_specs=(VM, VM),
        scratch_shapes=[
            pltpu.VMEM((128, 1024), BF16),
            pltpu.VMEM((1024, 2048), BF16),
            pltpu.SemaphoreType.DMA((5,)),
        ],
        compiler_params=params(14),
        cost_estimate=cost(2 * 128 * 1024 * 2048 * 4, 6 << 20),
        name="conv_out",
    )(parts, w)


def attn_out_kernel(parts, conv, w, out, rows):
    for c in range(8):
        rows[:, 128 * c : 128 * c + 128] = parts[c]
    for j in range(4):
        cols = slice(512 * j, 512 * j + 512)
        out[:, cols] = (dot(rows[...], w[:, cols]) + conv[:, cols]).astype(BF16)


def attn_out(parts, conv, w):
    return pl.pallas_call(
        attn_out_kernel,
        out_shape=jax.ShapeDtypeStruct((128, 2048), BF16),
        in_specs=[VM, VM, VM],
        out_specs=VM,
        scratch_shapes=[pltpu.VMEM((128, 1024), BF16)],
        compiler_params=params(10),
        cost_estimate=cost(2 * 128 * 1024 * 2048 * 4, 6 << 20),
        name="attn_out",
    )(parts, conv, w)


def layer(x, wq, wk, wv, wu, wg, taps, gain, gate, w_out):
    x, wq, wk, wv, wu, wg, w_out = (
        pltpu.with_memory_space_constraint(v, pltpu.HBM) for v in (x, wq, wk, wv, wu, wg, w_out)
    )
    own = lax.axis_index("sp").astype(I32).reshape(1)
    table = jnp.asarray(work_table())
    px, pz, tail = project(x, wq, wk, wv, wu, wg, gate.reshape(8, 128))
    halo = lax.ppermute(tail, "sp", [(i, i + 1) for i in range(15)])
    xs, zs = [None] * 4, [None] * 4
    for d in (1, 3, 2):
        xs[d] = lax.ppermute(px, "sp", moves(-d, 0))
        zs[d] = lax.ppermute(pz, "sp", moves(0, -d))
    gated = glu(x, wu, wg, px)
    conv = convolve(gated, halo, taps, gain.reshape(1, 128))
    conv_parts = lax.all_to_all(conv, "tp", 0, 0, tiled=True)
    conv_mixed, w_attn = conv_out(conv_parts, w_out)
    state = diagonal(px, pz)
    near = (px, xs[1], xs[3], pz, zs[1], zs[3])
    state = attend_near(table, own, near, state, conv_mixed)
    packs = (px, *xs[1:], pz, *zs[1:])
    o_own, lse_own, *sent = attend_far(table, own, packs, state)
    backs = [lax.ppermute(sent[d - 1], "sp", moves(d, 0)) for d in (1, 2, 3)]
    backs += [lax.ppermute(sent[d + 2], "sp", moves(0, d)) for d in (1, 2, 3)]
    mixed = combine(o_own, lse_own, backs)
    attn_parts = lax.all_to_all(mixed, "tp", 0, 0, tiled=True)
    return attn_out(attn_parts, conv_mixed, w_attn)


def solution(mesh):
    in_specs = (
        P("sp", None),
        P(None, "tp"),
        P(None, "tp"),
        P(None, "tp"),
        P(None, "tp"),
        P(None, "tp"),
        P(None, "tp"),
        P("tp"),
        P("sp", "tp"),
        P(),
    )
    out_specs = P(("sp", "tp"), None)
    return jax.shard_map(
        layer, mesh=mesh, in_specs=in_specs, out_specs=out_specs, check_vma=False
    )
```

```python
import functools

import jax
import jax.numpy as jnp
import numpy as np
from jax import lax
from jax.experimental import pallas as pl
from jax.experimental.pallas import tpu as pltpu
from jax.sharding import PartitionSpec as P


BF16, F32, I32 = jnp.bfloat16, jnp.float32, jnp.int32
SIDE = 4
HEAD = 128
TOK = 1024
HALF = 512
TAPS = 31
GATE_ROW = TOK
QUERY_ROW = TOK + 16
PACK_ROWS = QUERY_ROW + HALF // 2
BACK_ROWS = HALF + 16
TILES = 15
LOG2E = 1.4426950408889634
SCALE = HEAD**-0.5 * LOG2E
LOW = -1e30
TINY = 1e-37
EPS = 1e-05

VM = pl.BlockSpec(memory_space=pltpu.VMEM)
SM = pl.BlockSpec(memory_space=pltpu.SMEM)
ANY = pl.BlockSpec(memory_space=pl.ANY)
HBM = pl.BlockSpec(memory_space=pltpu.HBM)


def dot(a, b):
    return jnp.dot(a, b, preferred_element_type=F32)


def params(mib):
    return pltpu.CompilerParams(vmem_limit_bytes=mib << 20)


def cost(flops, moved):
    return pl.CostEstimate(flops=flops, bytes_accessed=moved, transcendentals=0)


def moves(dx, dz):
    return [
        (z * SIDE + x, (z + dz) % SIDE * SIDE + (x + dx) % SIDE)
        for z in range(SIDE)
        for x in range(SIDE)
    ]


def eye():
    return lax.broadcasted_iota(I32, (128, 128), 0) == lax.broadcasted_iota(I32, (128, 128), 1)


def to_row(column):
    return jnp.sum(jnp.where(eye(), column, 0.0), axis=0, keepdims=True)


def to_column(row):
    return jnp.sum(jnp.where(eye(), row, 0.0), axis=1, keepdims=True)


def split3(value):
    top = value.astype(BF16)
    rest = value - top.astype(F32)
    mid = rest.astype(BF16)
    return top, mid, (rest - mid.astype(F32)).astype(BF16)


def work_table():
    table = np.zeros((SIDE * SIDE, 2, TILES + 1), np.int32)
    for z in range(SIDE):
        for x in range(SIDE):
            tiles = []
            for d in range(SIDE):
                for e in range(SIDE):
                    late = d == 2 or e == 2
                    first_z = (z + e) % SIDE
                    if first_z < z or (e == 0 and x < (x + d) % SIDE):
                        tiles.append((late, d, 4 + e if e else 0))
                    second_z = (z + d) % SIDE
                    if second_z > z or (d == 0 and (x + e) % SIDE < x):
                        tiles.append((late, 4 + d, e))
            assert len(tiles) == TILES and sum(not t[0] for t in tiles) == 8
            for n, (_, q, k) in enumerate(sorted(tiles)):
                table[z * SIDE + x, :, n] = q, k
    return table


def gate_rows(both):
    return (both[:, :128] * jax.nn.sigmoid(both[:, 128:])).astype(BF16)


def project_kernel(x_hbm, wq, wk, wv, wu, wg, gate, px, pz, gated, tail, x, w, sems):
    arrivals = [
        pltpu.make_async_copy(
            x_hbm.at[pl.ds(256 * i, 256)], x.at[pl.ds(256 * i, 256)], sems.at[i]
        )
        for i in range(4)
    ]
    loads = [
        pltpu.make_async_copy(source, w.at[:, pl.ds(128 * n, 128)], sems.at[4 + n])
        for n, source in enumerate((wk, wv, wq, wu, wg))
    ]
    for c in (*loads[:3], *arrivals, *loads[3:]):
        c.start()
    zero = jnp.zeros((8, 128), BF16)
    top, mid, low = split3(gate[...] * (-LOG2E))
    gates = jnp.concatenate(
        [jnp.concatenate([top, mid], axis=1), jnp.concatenate([low, zero], axis=1)], axis=0
    )
    px[GATE_ROW : GATE_ROW + 16, :] = gates
    pz[GATE_ROW : GATE_ROW + 16, :] = gates
    for c in loads[:3]:
        c.wait()
    for i in range(4):
        arrivals[i].wait()
        out = dot(x[256 * i : 256 * i + 256, :], w[:, :384])
        both = out[:, :256].astype(BF16)
        px[256 * i : 256 * i + 256, :] = both
        pz[256 * i : 256 * i + 256, :] = both
        dest = px if i < 2 else pz
        lane = 128 * (i % 2)
        dest[QUERY_ROW:PACK_ROWS, lane : lane + 128] = (out[:, 256:] * SCALE).astype(BF16)
    for c in loads[3:]:
        c.wait()
    for i in range(4):
        rows = gate_rows(dot(x[256 * i : 256 * i + 256, :], w[:, 384:]))
        gated[256 * i : 256 * i + 256, :] = rows
    tail[...] = rows[224:, :]


def project(x, wq, wk, wv, wu, wg, gate):
    pack = jax.ShapeDtypeStruct((PACK_ROWS, 256), BF16)
    return pl.pallas_call(
        project_kernel,
        out_shape=(
            pack,
            pack,
            jax.ShapeDtypeStruct((TOK, 128), BF16),
            jax.ShapeDtypeStruct((32, 128), BF16),
        ),
        in_specs=[HBM] * 6 + [VM],
        out_specs=(VM,) * 4,
        scratch_shapes=[
            pltpu.VMEM((TOK, 2048), BF16),
            pltpu.VMEM((2048, 640), BF16),
            pltpu.SemaphoreType.DMA((9,)),
        ],
        compiler_params=params(12),
        cost_estimate=cost(2 * TOK * 2048 * 640, 8 << 20),
        name="project",
    )(x, wq, wk, wv, wu, wg, gate)


def conv_kernel(gated, halo, taps, gain, out, padded):
    padded[0:32, :] = halo[...].astype(F32)
    padded[32 : 32 + TOK, :] = gated[...].astype(F32)
    padded[32 + TOK :, :] = jnp.zeros((8, 128), F32)
    for block in range(8):
        start = 128 * block
        total = None
        for r in range(8):
            part = None
            for q in range(5):
                j = 8 * q + r - 2
                if 0 <= j < TAPS:
                    term = taps[j : j + 1, :] * padded[start + 8 * q : start + 8 * q + 136, :]
                    part = term if part is None else part + term
            part = part[r : r + 128, :]
            total = part if total is None else total + part
        out[block, 0:128, :] = total
        out[block, 128:136, :] = jnp.broadcast_to(gain[...], (8, 128))


def convolve(gated, halo, taps, gain):
    return pl.pallas_call(
        conv_kernel,
        out_shape=jax.ShapeDtypeStruct((8, 136, 128), F32),
        in_specs=[VM] * 4,
        out_specs=VM,
        scratch_shapes=[pltpu.VMEM((TOK + 40, 128), F32)],
        compiler_params=params(8),
        cost_estimate=cost(2 * TOK * 128 * 31 * 64, 1 << 20),
        name="convolve",
    )(gated, halo, taps, gain)


def diagonal(px, pz, m, l, acc):
    top = px[GATE_ROW : GATE_ROW + 8, :].astype(F32)
    low = px[GATE_ROW + 8 : GATE_ROW + 16, :].astype(F32)
    gates = top[:, :128] + top[:, 128:] + low[:, :128]
    for half, pack in ((0, px), (1, pz)):
        keys = HALF * (half + 1)
        query = jnp.concatenate(
            [pack[QUERY_ROW:PACK_ROWS, :128], pack[QUERY_ROW:PACK_ROWS, 128:]], axis=0
        )
        scores = lax.dot_general(
            query, px[:keys, :128], (((1,), (1,)), ((), ())), preferred_element_type=F32
        )
        row = lax.broadcasted_iota(I32, (HALF, 128), 0) + HALF * half
        lane = lax.broadcasted_iota(I32, (HALF, 128), 1)
        parts = []
        for c in range(keys // 128):
            t = scores[:, 128 * c : 128 * c + 128] + gates[c : c + 1, :]
            parts.append(jnp.where(lane + 128 * c <= row, t, LOW))
        most = functools.reduce(jnp.maximum, parts)
        most = jnp.broadcast_to(jnp.max(most, axis=1, keepdims=True), (HALF, 128))
        weights = [jnp.exp2(t - most) for t in parts]
        m[4 * half] = most
        rounded = jnp.concatenate([w.astype(BF16) for w in weights], axis=1)
        ones = jnp.ones((keys, 128), BF16)
        out = dot(rounded, jnp.concatenate([px[:keys, 128:], ones], axis=1))
        acc[4 * half] = out[:, :128]
        l[4 * half] = out[:, 128:]


PACKS = 8
NEAR, FAR = 8, 7


def start_packs(sources, packs, sems):
    rows = PACK_ROWS // 3
    copies = [
        pltpu.make_async_copy(
            src.at[pl.ds(rows * i, rows)], packs.at[n, pl.ds(rows * i, rows)], sems.at[3 * n + i]
        )
        for n, src in sources
        for i in range(3)
    ]
    for c in copies:
        c.start()
    return copies


def finish_packs(copies, sources, packs, query, gates):
    for c in copies:
        c.wait()
    for slot, _ in sources:
        for side in range(2):
            query[slot, 256 * side : 256 * side + 256, :] = packs[
                slot, QUERY_ROW:PACK_ROWS, 128 * side : 128 * side + 128
            ]
        top = packs[slot, GATE_ROW : GATE_ROW + 8, :].astype(F32)
        low = packs[slot, GATE_ROW + 8 : GATE_ROW + 16, :].astype(F32)
        gates[slot] = top[:, :128] + top[:, 128:] + low[:, :128]


def run_tiles(table, own, start, count, packs, query, gates, per_tile, m, l, acc):
    sa, sb, ma, mb, aa, ab = per_tile
    row = own[0]
    first, second = (sa, ma, aa), (sb, mb, ab)

    def scores_of(n, s, most, shrink):
        q, k = table[row, 0, n], table[row, 1, n]
        raw = lax.dot_general(
            query[q], packs[k, :TOK, :128], (((1,), (1,)), ((), ())), preferred_element_type=F32
        )
        best = None
        for c in range(8):
            t = raw[:, 128 * c : 128 * c + 128] + gates[k, c : c + 1, :]
            s[:, 128 * c : 128 * c + 128] = t
            best = t if best is None else jnp.maximum(best, t)
        old = m[q]
        new = jnp.maximum(old, jnp.max(best, axis=1, keepdims=True))
        shrink[...] = jnp.exp2(old - new)
        m[q] = new
        most[...] = new

    def weigh(n, s, most, shrink):
        q, k = table[row, 0, n], table[row, 1, n]
        top = most[...]
        by = shrink[...]
        w = [jnp.exp2(s[:, 128 * c : 128 * c + 128] - top) for c in range(8)]
        rounded = jnp.concatenate([v.astype(BF16) for v in w], axis=1)
        ones = jnp.ones((TOK, 128), BF16)
        out = dot(rounded, jnp.concatenate([packs[k, :TOK, 128:], ones], axis=1))
        acc[q] = acc[q] * by + out[:, :128]
        l[q] = l[q] * by + out[:, 128:]


    scores_of(start, *first)

    def two_tiles(i, carry):
        n = start + 2 * i
        scores_of(n + 1, *second)
        weigh(n, *first)
        scores_of(n + 2, *first)
        weigh(n + 1, *second)
        return carry

    lax.fori_loop(0, (count - 1) // 2, two_tiles, 0)
    if count % 2 == 0:
        scores_of(start + count - 1, *second)
        weigh(start + count - 2, *first)
        weigh(start + count - 1, *second)
    else:
        weigh(start + count - 1, *first)


def near_kernel(
    table, own, px, x1, x3, pz, z1, z3, m, l, acc, packs, query, gates, sems, *per_tile
):
    sources = ((0, px), (1, x1), (3, x3), (4, pz), (5, z1), (7, z3))
    copies = start_packs(sources, packs, sems)
    for n in (1, 3, 5, 7):
        m[n] = jnp.full((HALF, 128), LOW, F32)
        l[n] = jnp.zeros((HALF, 128), F32)
        acc[n] = jnp.zeros((HALF, 128), F32)
    diagonal(px, pz, m, l, acc)
    finish_packs(copies, sources, packs, query, gates)
    run_tiles(table, own, 0, NEAR, packs, query, gates, per_tile, m, l, acc)


def far_kernel(
    table, own, x2, z2, m_in, l_in, acc_in, packs_in, query_in, gates_in,
    o_own, lse_own, a1, a2, a3, b1, b2, b3,
    packs, query, gates, sems, m, l, acc, *per_tile,
):
    sources = ((2, x2), (6, z2))
    copies = start_packs(sources, packs, sems)
    for n in (0, 1, 3, 4, 5, 7):
        if n != 4:
            packs[n, :TOK, :] = packs_in[n, :TOK, :]
        query[n] = query_in[n]
        gates[n] = gates_in[n]
        m[n] = m_in[n]
        l[n] = l_in[n]
        acc[n] = acc_in[n]
    for n in (2, 6):
        m[n] = jnp.full((HALF, 128), LOW, F32)
        l[n] = jnp.zeros((HALF, 128), F32)
        acc[n] = jnp.zeros((HALF, 128), F32)
    finish_packs(copies, sources, packs, query, gates)
    run_tiles(table, own, NEAR, FAR, packs, query, gates, per_tile, m, l, acc)
    for n, out in enumerate((None, a1, a2, a3, None, b1, b2, b3)):
        total = jnp.maximum(l[n], TINY)
        mixed = acc[n] / total
        lse = m[n] + jnp.log2(total)
        if out is None:
            o_own[n // 4] = mixed
            lse_own[n // 4] = lse
        else:
            out[0:HALF, :] = mixed.astype(BF16)
            rows = [to_row(lse[128 * b : 128 * b + 128, :]) for b in range(4)]
            parts = split3(jnp.concatenate(rows + rows, axis=0))
            out[HALF : HALF + 16, :] = jnp.concatenate(
                [parts[0][:4], parts[1][:4], parts[2]], axis=0
            )


SEMS = [pltpu.SemaphoreType.DMA((3 * PACKS,))]
SLOTS = [
    ((PACKS, PACK_ROWS, 256), BF16),
    ((PACKS, HALF, 128), BF16),
    ((PACKS, 8, 128), F32),
]
STATE = [((PACKS, HALF, 128), F32)] * 3
TILE = [((HALF, TOK), F32)] * 2 + [((HALF, 128), F32)] * 4


def arrays(shapes):
    return tuple(jax.ShapeDtypeStruct(*v) for v in shapes)


def scratch(shapes):
    return [pltpu.VMEM(*v) for v in shapes]


def attend_near(table, own, packs):
    return pl.pallas_call(
        near_kernel,
        out_shape=arrays(STATE + SLOTS),
        in_specs=[SM, SM, VM, ANY, ANY, VM, ANY, ANY],
        out_specs=(VM,) * 6,
        scratch_shapes=SEMS + scratch(TILE),
        compiler_params=params(24),
        cost_estimate=cost(NEAR * 4 * HALF * TOK * 256, 8 << 20),
        name="attend_near",
    )(table, own, *packs)


def attend_far(table, own, x2, z2, state):
    outs = [((2, HALF, 128), F32)] * 2 + [((BACK_ROWS, 128), BF16)] * 6
    return pl.pallas_call(
        far_kernel,
        out_shape=arrays(outs),
        in_specs=[SM, SM, ANY, ANY] + [VM] * 6,
        out_specs=(VM,) * 8,
        scratch_shapes=scratch(SLOTS) + SEMS + scratch(STATE + TILE),
        compiler_params=params(30),
        cost_estimate=cost(FAR * 4 * HALF * TOK * 256, 8 << 20),
        name="attend_far",
    )(table, own, x2, z2, *state)


def combine_kernel(o_own, lse_own, a1, a2, a3, b1, b2, b3, out):
    for half, backs in ((0, (a1, a2, a3)), (1, (b1, b2, b3))):
        lses = []
        for back in backs:
            tail = back[HALF : HALF + 16, :].astype(F32)
            lses.append(tail[0:4] + tail[4:8] + tail[8:12])
        for b in range(4):
            rows = slice(128 * b, 128 * b + 128)
            columns = [lse_own[half, rows, :]]
            columns += [jnp.broadcast_to(to_column(v[b : b + 1, :]), (128, 128)) for v in lses]
            most = functools.reduce(jnp.maximum, columns)
            shares = [jnp.exp2(c - most) for c in columns]
            mixed = shares[0] * o_own[half, rows, :]
            for share, back in zip(shares[1:], backs):
                mixed = mixed + share * back[rows, :].astype(F32)
            out[4 * half + b] = (mixed / functools.reduce(jnp.add, shares)).astype(BF16)


def combine(o_own, lse_own, backs):
    return pl.pallas_call(
        combine_kernel,
        out_shape=jax.ShapeDtypeStruct((8, 128, 128), BF16),
        in_specs=[VM] * 8,
        out_specs=VM,
        compiler_params=params(16),
        cost_estimate=cost(1 << 29, 2 << 20),
        name="combine",
    )(o_own, lse_own, *backs)


def conv_out_kernel(parts, w_hbm, out, later, rows, w, sems):
    copies = []
    for j in range(4):
        cols = pl.ds(512 * j, 512)
        copies.append(
            pltpu.make_async_copy(w_hbm.at[pl.ds(0, 1024), cols], w.at[:, cols], sems.at[j])
        )
    copies.append(pltpu.make_async_copy(w_hbm.at[pl.ds(1024, 1024)], later, sems.at[4]))
    for c in copies:
        c.start()
    total = functools.reduce(jnp.add, [parts[c, :128, :] for c in range(8)])
    mean = jnp.sum(total, axis=1, keepdims=True) * (1.0 / 1024)
    far = [parts[c, :128, :] - mean for c in range(8)]
    spread = functools.reduce(jnp.add, [v * v for v in far])
    spread = jnp.sum(spread, axis=1, keepdims=True) * (1.0 / 1024)
    inverse = lax.rsqrt(spread + EPS)
    for c in range(8):
        v = far[c] * inverse * parts[c, 128:129, :]
        rows[:, 128 * c : 128 * c + 128] = (v * jax.nn.sigmoid(v)).astype(BF16)
    for j in range(4):
        copies[j].wait()
        out[:, 512 * j : 512 * j + 512] = dot(rows[...], w[:, 512 * j : 512 * j + 512])
    copies[4].wait()


def conv_out(parts, w):
    return pl.pallas_call(
        conv_out_kernel,
        out_shape=(
            jax.ShapeDtypeStruct((128, 2048), F32),
            jax.ShapeDtypeStruct((1024, 2048), BF16),
        ),
        in_specs=[VM, HBM],
        out_specs=(VM, VM),
        scratch_shapes=[
            pltpu.VMEM((128, 1024), BF16),
            pltpu.VMEM((1024, 2048), BF16),
            pltpu.SemaphoreType.DMA((5,)),
        ],
        compiler_params=params(14),
        cost_estimate=cost(2 * 128 * 1024 * 2048 * 4, 6 << 20),
        name="conv_out",
    )(parts, w)


def attn_out_kernel(parts, conv, w, out, rows):
    for c in range(8):
        rows[:, 128 * c : 128 * c + 128] = parts[c]
    for j in range(4):
        cols = slice(512 * j, 512 * j + 512)
        out[:, cols] = (dot(rows[...], w[:, cols]) + conv[:, cols]).astype(BF16)


def attn_out(parts, conv, w):
    return pl.pallas_call(
        attn_out_kernel,
        out_shape=jax.ShapeDtypeStruct((128, 2048), BF16),
        in_specs=[VM, VM, VM],
        out_specs=VM,
        scratch_shapes=[pltpu.VMEM((128, 1024), BF16)],
        compiler_params=params(10),
        cost_estimate=cost(2 * 128 * 1024 * 2048 * 4, 6 << 20),
        name="attn_out",
    )(parts, conv, w)


def layer(x, wq, wk, wv, wu, wg, taps, gain, gate, w_out):
    x, wq, wk, wv, wu, wg, w_out = (
        pltpu.with_memory_space_constraint(v, pltpu.HBM) for v in (x, wq, wk, wv, wu, wg, w_out)
    )
    own = lax.axis_index("sp").astype(I32).reshape(1)
    table = jnp.asarray(work_table())
    px, pz, gated, tail = project(x, wq, wk, wv, wu, wg, gate.reshape(8, 128))
    halo = lax.ppermute(tail, "sp", [(i, i + 1) for i in range(15)])
    xs, zs = [None] * 4, [None] * 4
    for d in (1, 3, 2):
        xs[d] = lax.ppermute(px, "sp", moves(-d, 0))
        zs[d] = lax.ppermute(pz, "sp", moves(0, -d))
    conv = convolve(gated, halo, taps, gain.reshape(1, 128))
    conv_parts = lax.all_to_all(conv, "tp", 0, 0, tiled=True)
    near = (px, xs[1], xs[3], pz, zs[1], zs[3])
    state = attend_near(table, own, near)
    o_own, lse_own, *sent = attend_far(table, own, xs[2], zs[2], state)
    backs = [
        lax.ppermute(sent[n], "sp", moves(*move))
        for n, move in enumerate(((1, 0), (2, 0), (3, 0), (0, 1), (0, 2), (0, 3)))
    ]
    conv_mixed, w_attn = conv_out(conv_parts, w_out)
    mixed = combine(o_own, lse_own, backs)
    attn_parts = lax.all_to_all(mixed, "tp", 0, 0, tiled=True)
    return attn_out(attn_parts, conv_mixed, w_attn)


def solution(mesh):
    in_specs = (
        P("sp", None),
        P(None, "tp"),
        P(None, "tp"),
        P(None, "tp"),
        P(None, "tp"),
        P(None, "tp"),
        P(None, "tp"),
        P("tp"),
        P("sp", "tp"),
        P(),
    )
    out_specs = P(("sp", "tp"), None)
    return jax.shard_map(
        layer, mesh=mesh, in_specs=in_specs, out_specs=out_specs, check_vma=False
    )
```

```python
import functools

import jax
import jax.numpy as jnp
import numpy as np
from jax import lax
from jax.experimental import pallas as pl
from jax.experimental.pallas import tpu as pltpu
from jax.sharding import PartitionSpec as P


BF16, F32, I32 = jnp.bfloat16, jnp.float32, jnp.int32
SIDE = 4
HEAD = 128
TOK = 1024
HALF = 512
TAPS = 31
GATE_ROW = TOK
PACK_ROWS = TOK + 16
BACK_ROWS = HALF + 16
TILES = 15
LOG2E = 1.4426950408889634
SCALE = HEAD**-0.5 * LOG2E
LOW = -1e30
TINY = 1e-37
EPS = 1e-05

VM = pl.BlockSpec(memory_space=pltpu.VMEM)
SM = pl.BlockSpec(memory_space=pltpu.SMEM)
ANY = pl.BlockSpec(memory_space=pl.ANY)
HBM = pl.BlockSpec(memory_space=pltpu.HBM)


def dot(a, b):
    return jnp.dot(a, b, preferred_element_type=F32)


def params(mib):
    return pltpu.CompilerParams(vmem_limit_bytes=mib << 20)


def cost(flops, moved):
    return pl.CostEstimate(flops=flops, bytes_accessed=moved, transcendentals=0)


def moves(dx, dz):
    return [
        (z * SIDE + x, (z + dz) % SIDE * SIDE + (x + dx) % SIDE)
        for z in range(SIDE)
        for x in range(SIDE)
    ]


def eye():
    return lax.broadcasted_iota(I32, (128, 128), 0) == lax.broadcasted_iota(I32, (128, 128), 1)


def to_row(column):
    return jnp.sum(jnp.where(eye(), column, 0.0), axis=0, keepdims=True)


def to_column(row):
    return jnp.sum(jnp.where(eye(), row, 0.0), axis=1, keepdims=True)


def split3(value):
    top = value.astype(BF16)
    rest = value - top.astype(F32)
    mid = rest.astype(BF16)
    return top, mid, (rest - mid.astype(F32)).astype(BF16)


UP_HALVES = np.array([[0, 0, 0, 1], [0, 0, 1, 2], [0, 1, 2, 2], [1, 2, 2, 2]])


def work_table():
    table = np.zeros((SIDE * SIDE, 3, TILES + 1), np.int32)
    for z in range(SIDE):
        for x in range(SIDE):
            tiles = []
            for d in range(SIDE):
                other = (x + d) % SIDE
                late = d == 2
                for h in range(2):
                    if z < 2:
                        tiles.append((late, 2 + h, d))
                        if other < x:
                            tiles.append((late, h, d))
                        if h < 2 - UP_HALVES[x, other]:
                            tiles.append((late, 4 + h, d))
                    else:
                        tiles.append((late, 2 * d + h, 2))
                        if other > x:
                            tiles.append((late, 2 * d + h, 0))
                        if h >= 2 - UP_HALVES[other, x]:
                            tiles.append((late, 2 * d + h, 1))
            near = sum(not t[0] for t in tiles)
            assert len(tiles) == TILES and near % 2 == 1
            for n, (_, q, k) in enumerate(sorted(tiles)):
                table[z * SIDE + x, :2, n] = q, k
            table[z * SIDE + x, 2, 0] = near
    return table


def gate_rows(both):
    return (both[:, :128] * jax.nn.sigmoid(both[:, 128:])).astype(BF16)


def project_kernel(
    own, x_hbm, wq, wk, wv, wu, wg, gate, pkv, pxx, pq, gated, tail, x, w, sems
):
    low_level = own[0] < 8
    arrivals = [
        pltpu.make_async_copy(
            x_hbm.at[pl.ds(256 * i, 256)], x.at[pl.ds(256 * i, 256)], sems.at[i]
        )
        for i in range(4)
    ]
    loads = [
        pltpu.make_async_copy(source, w.at[:, pl.ds(128 * n, 128)], sems.at[4 + n])
        for n, source in enumerate((wk, wv, wq, wu, wg))
    ]
    for c in (*loads[:3], *arrivals, *loads[3:]):
        c.start()
    zero = jnp.zeros((8, 128), BF16)
    top, mid, low = split3(gate[...] * (-LOG2E))
    gates = jnp.concatenate(
        [jnp.concatenate([top, mid], axis=1), jnp.concatenate([low, zero], axis=1)], axis=0
    )
    pkv[GATE_ROW : GATE_ROW + 16, :] = gates
    pxx[GATE_ROW : GATE_ROW + 16, :] = gates
    for c in loads[:3]:
        c.wait()
    for i in range(4):
        arrivals[i].wait()
        out = dot(x[256 * i : 256 * i + 256, :], w[:, :384])
        both = out[:, :256].astype(BF16)
        query = (out[:, 256:] * SCALE).astype(BF16)
        rows = slice(256 * i, 256 * i + 256)
        half = slice(256 * (i % 2), 256 * (i % 2) + 256)
        lanes = slice(128 * (i // 2), 128 * (i // 2) + 128)
        pkv[rows, :] = both
        pq[half, lanes] = query
        if i >= 2:
            pxx[rows, :] = both
        else:

            @pl.when(low_level)
            def _():
                pxx[rows, :] = both

        @pl.when(jnp.logical_not(low_level))
        def _():
            pxx[half, lanes] = query

    for c in loads[3:]:
        c.wait()
    for i in range(4):
        rows = gate_rows(dot(x[256 * i : 256 * i + 256, :], w[:, 384:]))
        gated[256 * i : 256 * i + 256, :] = rows
    tail[...] = rows[224:, :]


def project(own, x, wq, wk, wv, wu, wg, gate):
    pack = jax.ShapeDtypeStruct((PACK_ROWS, 256), BF16)
    return pl.pallas_call(
        project_kernel,
        out_shape=(
            pack,
            pack,
            jax.ShapeDtypeStruct((HALF, 256), BF16),
            jax.ShapeDtypeStruct((TOK, 128), BF16),
            jax.ShapeDtypeStruct((32, 128), BF16),
        ),
        in_specs=[SM] + [HBM] * 6 + [VM],
        out_specs=(VM,) * 5,
        scratch_shapes=[
            pltpu.VMEM((TOK, 2048), BF16),
            pltpu.VMEM((2048, 640), BF16),
            pltpu.SemaphoreType.DMA((9,)),
        ],
        compiler_params=params(12),
        cost_estimate=cost(2 * TOK * 2048 * 640, 8 << 20),
        name="project",
    )(own, x, wq, wk, wv, wu, wg, gate)


def conv_kernel(gated, halo, taps, gain, out, padded):
    padded[0:32, :] = halo[...].astype(F32)
    padded[32 : 32 + TOK, :] = gated[...].astype(F32)
    padded[32 + TOK :, :] = jnp.zeros((8, 128), F32)
    for block in range(8):
        start = 128 * block
        total = None
        for r in range(8):
            part = None
            for q in range(5):
                j = 8 * q + r - 2
                if 0 <= j < TAPS:
                    term = taps[j : j + 1, :] * padded[start + 8 * q : start + 8 * q + 136, :]
                    part = term if part is None else part + term
            part = part[r : r + 128, :]
            total = part if total is None else total + part
        out[block, 0:128, :] = total
        out[block, 128:136, :] = jnp.broadcast_to(gain[...], (8, 128))


def convolve(gated, halo, taps, gain):
    return pl.pallas_call(
        conv_kernel,
        out_shape=jax.ShapeDtypeStruct((8, 136, 128), F32),
        in_specs=[VM] * 4,
        out_specs=VM,
        scratch_shapes=[pltpu.VMEM((TOK + 40, 128), F32)],
        compiler_params=params(8),
        cost_estimate=cost(2 * TOK * 128 * 31 * 64, 1 << 20),
        name="convolve",
    )(gated, halo, taps, gain)


def diagonal(pkv, pq, m, l, acc):
    top = pkv[GATE_ROW : GATE_ROW + 8, :].astype(F32)
    low = pkv[GATE_ROW + 8 : GATE_ROW + 16, :].astype(F32)
    gates = top[:, :128] + top[:, 128:] + low[:, :128]
    for half in range(2):
        keys = HALF * (half + 1)
        scores = lax.dot_general(
            pq[:, 128 * half : 128 * half + 128],
            pkv[:keys, :128],
            (((1,), (1,)), ((), ())),
            preferred_element_type=F32,
        )
        row = lax.broadcasted_iota(I32, (HALF, 128), 0) + HALF * half
        lane = lax.broadcasted_iota(I32, (HALF, 128), 1)
        parts = []
        for c in range(keys // 128):
            t = scores[:, 128 * c : 128 * c + 128] + gates[c : c + 1, :]
            parts.append(jnp.where(lane + 128 * c <= row, t, LOW))
        most = functools.reduce(jnp.maximum, parts)
        most = jnp.broadcast_to(jnp.max(most, axis=1, keepdims=True), (HALF, 128))
        weights = [jnp.exp2(t - most) for t in parts]
        m[half] = most
        rounded = jnp.concatenate([w.astype(BF16) for w in weights], axis=1)
        ones = jnp.ones((keys, 128), BF16)
        out = dot(rounded, jnp.concatenate([pkv[:keys, 128:], ones], axis=1))
        acc[half] = out[:, :128]
        l[half] = out[:, 128:]


QUERIES = 8


def key_copies(source, packs, slot, sems):
    return [
        pltpu.make_async_copy(
            source.at[pl.ds(at, rows)], packs.at[slot, pl.ds(at, rows)], sems.at[n, slot]
        )
        for n, (at, rows) in enumerate(((0, HALF), (HALF, PACK_ROWS - HALF)))
    ]


def query_copy(source, qpacks, slot, sems):
    return pltpu.make_async_copy(source.at[pl.ds(0, HALF)], qpacks.at[slot], sems.at[2, slot])


def unpack_keys(packs, slots, gates):
    for n in slots:
        top = packs[n, GATE_ROW : GATE_ROW + 8, :].astype(F32)
        low = packs[n, GATE_ROW + 8 : GATE_ROW + 16, :].astype(F32)
        gates[n] = top[:, :128] + top[:, 128:] + low[:, :128]


def unpack_queries(qpacks, slots, query):
    for n in slots:
        query[2 * n] = qpacks[n, :, :128]
        query[2 * n + 1] = qpacks[n, :, 128:]


def each(copies, action):
    for c in copies:
        getattr(c, action)()


def finish(m, l, acc, first, out):
    for n in range(2):
        total = jnp.maximum(l[first + n], TINY)
        lse = m[first + n] + jnp.log2(total)
        base = BACK_ROWS * n
        out[base : base + HALF, :] = (acc[first + n] / total).astype(BF16)
        rows = [to_row(lse[128 * b : 128 * b + 128, :]) for b in range(4)]
        parts = split3(jnp.concatenate(rows + rows, axis=0))
        out[base + HALF : base + BACK_ROWS, :] = jnp.concatenate(
            [parts[0][:4], parts[1][:4], parts[2]], axis=0
        )


def run_tiles(table, own, start, count, even, packs, query, gates, per_tile, m, l, acc):
    sa, sb, ma, mb, aa, ab = per_tile
    row = own[0]
    first, second = (sa, ma, aa), (sb, mb, ab)

    def scores_of(n, s, most, shrink):
        q, k = table[row, 0, n], table[row, 1, n]
        raw = lax.dot_general(
            query[q], packs[k, :TOK, :128], (((1,), (1,)), ((), ())), preferred_element_type=F32
        )
        best = None
        for c in range(8):
            t = raw[:, 128 * c : 128 * c + 128] + gates[k, c : c + 1, :]
            s[:, 128 * c : 128 * c + 128] = t
            best = t if best is None else jnp.maximum(best, t)
        old = m[q]
        new = jnp.maximum(old, jnp.max(best, axis=1, keepdims=True))
        shrink[...] = jnp.exp2(old - new)
        m[q] = new
        most[...] = new

    def weigh(n, s, most, shrink):
        q, k = table[row, 0, n], table[row, 1, n]
        top = most[...]
        by = shrink[...]
        w = [jnp.exp2(s[:, 128 * c : 128 * c + 128] - top) for c in range(8)]
        rounded = jnp.concatenate([v.astype(BF16) for v in w], axis=1)
        ones = jnp.ones((TOK, 128), BF16)
        out = dot(rounded, jnp.concatenate([packs[k, :TOK, 128:], ones], axis=1))
        acc[q] = acc[q] * by + out[:, :128]
        l[q] = l[q] * by + out[:, 128:]


    scores_of(start, *first)

    def two_tiles(i, carry):
        n = start + 2 * i
        scores_of(n + 1, *second)
        weigh(n, *first)
        scores_of(n + 2, *first)
        weigh(n + 1, *second)
        return carry

    lax.fori_loop(0, (count - 1) // 2, two_tiles, 0)
    if even:
        scores_of(start + count - 1, *second)
        weigh(start + count - 2, *first)
        weigh(start + count - 1, *second)
    else:
        weigh(start + count - 1, *first)


def near_kernel(
    table, own, pkv, pq, x1, x3, u, w, kx, ky,
    m, l, acc, packs, query, gates, b1, b3, qpacks, sems, *per_tile,
):
    low_level = own[0] < 8
    high_level = jnp.logical_not(low_level)
    low_copies = [
        *key_copies(x1, packs, 1, sems),
        *key_copies(x3, packs, 3, sems),
        query_copy(u, qpacks, 1, sems),
        query_copy(w, qpacks, 2, sems),
    ]
    high_copies = [
        *key_copies(kx, packs, 1, sems),
        *key_copies(ky, packs, 2, sems),
        query_copy(x1, qpacks, 1, sems),
        query_copy(x3, qpacks, 3, sems),
    ]
    pl.when(low_level)(lambda: each(low_copies, "start"))
    pl.when(high_level)(lambda: each(high_copies, "start"))
    for n in range(2, QUERIES):
        m[n] = jnp.full((HALF, 128), LOW, F32)
        l[n] = jnp.zeros((HALF, 128), F32)
        acc[n] = jnp.zeros((HALF, 128), F32)
    packs[0] = pkv[...]
    unpack_keys(packs, (0,), gates)
    query[0] = pq[:, :128]
    query[1] = pq[:, 128:]
    diagonal(pkv, pq, m, l, acc)

    @pl.when(low_level)
    def _():
        each(low_copies, "wait")
        unpack_keys(packs, (1, 3), gates)
        unpack_queries(qpacks, (1, 2), query)

    @pl.when(high_level)
    def _():
        each(high_copies, "wait")
        unpack_keys(packs, (1, 2), gates)
        unpack_queries(qpacks, (1, 3), query)

    count = table[own[0], 2, 0]
    run_tiles(table, own, 0, count, False, packs, query, gates, per_tile, m, l, acc)
    finish(m, l, acc, 2, b1)
    finish(m, l, acc, 6, b3)


def far_kernel(
    table, own, x2, m_in, l_in, acc_in, packs_in, query_in, gates_in,
    o_own, lse_own, b1, b2,
    m, l, acc, packs, query, gates, qpacks, sems, *per_tile,
):
    low_level = own[0] < 8
    high_level = jnp.logical_not(low_level)
    low_copies = key_copies(x2, packs, 2, sems)
    high_copies = [query_copy(x2, qpacks, 2, sems)]
    pl.when(low_level)(lambda: each(low_copies, "start"))
    pl.when(high_level)(lambda: each(high_copies, "start"))
    for n in range(6):
        m[n] = m_in[n]
        l[n] = l_in[n]
        acc[n] = acc_in[n]
        query[n] = query_in[n]
    for n in (0, 1, 3):
        packs[n, :TOK, :] = packs_in[n, :TOK, :]
        gates[n] = gates_in[n]

    @pl.when(low_level)
    def _():
        each(low_copies, "wait")
        unpack_keys(packs, (2,), gates)

    @pl.when(high_level)
    def _():
        packs[2, :TOK, :] = packs_in[2, :TOK, :]
        gates[2] = gates_in[2]
        each(high_copies, "wait")
        unpack_queries(qpacks, (2,), query)

    near = table[own[0], 2, 0]
    run_tiles(table, own, near, TILES - near, True, packs, query, gates, per_tile, m, l, acc)
    for n in range(2):
        total = jnp.maximum(l[n], TINY)
        o_own[n] = acc[n] / total
        lse_own[n] = m[n] + jnp.log2(total)
    finish(m, l, acc, 2, b1)
    finish(m, l, acc, 4, b2)


SEMS = [pltpu.SemaphoreType.DMA((3, 4))]
QPACKS = [((4, HALF, 256), BF16)]
SLOTS = [((4, PACK_ROWS, 256), BF16), ((QUERIES, HALF, 128), BF16), ((4, 8, 128), F32)]
STATE = [((QUERIES, HALF, 128), F32)] * 3
TILE = [((HALF, TOK), F32)] * 2 + [((HALF, 128), F32)] * 4
BACK = [((2 * BACK_ROWS, 128), BF16)]


def arrays(shapes):
    return tuple(jax.ShapeDtypeStruct(*v) for v in shapes)


def scratch(shapes):
    return [pltpu.VMEM(*v) for v in shapes]


def attend_near(table, own, *packs):
    return pl.pallas_call(
        near_kernel,
        out_shape=arrays(STATE + SLOTS + BACK * 2),
        in_specs=[SM, SM, VM, VM] + [ANY] * 6,
        out_specs=(VM,) * 8,
        scratch_shapes=scratch(QPACKS) + SEMS + scratch(TILE),
        compiler_params=params(24),
        cost_estimate=cost(12 * 4 * HALF * TOK * 256, 8 << 20),
        name="attend_near",
    )(table, own, *packs)


def attend_far(table, own, x2, state):
    return pl.pallas_call(
        far_kernel,
        out_shape=arrays([((2, HALF, 128), F32)] * 2 + BACK * 2),
        in_specs=[SM, SM, ANY] + [VM] * 6,
        out_specs=(VM,) * 4,
        scratch_shapes=scratch(STATE + SLOTS + QPACKS) + SEMS + scratch(TILE),
        compiler_params=params(30),
        cost_estimate=cost(5 * 4 * HALF * TOK * 256, 8 << 20),
        name="attend_far",
    )(table, own, x2, *state)


def combine_kernel(own, o_own, lse_own, x1, x2, x3, u, w, out):
    z = own[0] // SIDE
    high = z >= 2
    backs = ((x1, high), (x2, high), (x3, high), (u, z % 2 == 1), (w, high))
    for half in range(2):
        base = BACK_ROWS * half
        lses = []
        for back, there in backs:
            tail = back[base + HALF : base + BACK_ROWS, :].astype(F32)
            lses.append(jnp.where(there, tail[0:4] + tail[4:8] + tail[8:12], LOW))
        for b in range(4):
            rows = slice(128 * b, 128 * b + 128)
            columns = [lse_own[half, rows, :]]
            columns += [jnp.broadcast_to(to_column(v[b : b + 1, :]), (128, 128)) for v in lses]
            most = functools.reduce(jnp.maximum, columns)
            shares = [jnp.exp2(c - most) for c in columns]
            mixed = shares[0] * o_own[half, rows, :]
            for share, (back, _) in zip(shares[1:], backs):
                mixed = mixed + share * back[base + 128 * b : base + 128 * b + 128, :].astype(F32)
            out[4 * half + b] = (mixed / functools.reduce(jnp.add, shares)).astype(BF16)


def combine(own, o_own, lse_own, backs):
    return pl.pallas_call(
        combine_kernel,
        out_shape=jax.ShapeDtypeStruct((8, 128, 128), BF16),
        in_specs=[SM] + [VM] * 7,
        out_specs=VM,
        compiler_params=params(16),
        cost_estimate=cost(1 << 29, 2 << 20),
        name="combine",
    )(own, o_own, lse_own, *backs)


def conv_out_kernel(parts, w_hbm, out, later, rows, w, sems):
    copies = []
    for j in range(4):
        cols = pl.ds(512 * j, 512)
        copies.append(
            pltpu.make_async_copy(w_hbm.at[pl.ds(0, 1024), cols], w.at[:, cols], sems.at[j])
        )
    copies.append(pltpu.make_async_copy(w_hbm.at[pl.ds(1024, 1024)], later, sems.at[4]))
    for c in copies:
        c.start()
    total = functools.reduce(jnp.add, [parts[c, :128, :] for c in range(8)])
    mean = jnp.sum(total, axis=1, keepdims=True) * (1.0 / 1024)
    far = [parts[c, :128, :] - mean for c in range(8)]
    spread = functools.reduce(jnp.add, [v * v for v in far])
    spread = jnp.sum(spread, axis=1, keepdims=True) * (1.0 / 1024)
    inverse = lax.rsqrt(spread + EPS)
    for c in range(8):
        v = far[c] * inverse * parts[c, 128:129, :]
        rows[:, 128 * c : 128 * c + 128] = (v * jax.nn.sigmoid(v)).astype(BF16)
    for j in range(4):
        copies[j].wait()
        out[:, 512 * j : 512 * j + 512] = dot(rows[...], w[:, 512 * j : 512 * j + 512])
    copies[4].wait()


def conv_out(parts, w):
    return pl.pallas_call(
        conv_out_kernel,
        out_shape=(
            jax.ShapeDtypeStruct((128, 2048), F32),
            jax.ShapeDtypeStruct((1024, 2048), BF16),
        ),
        in_specs=[VM, HBM],
        out_specs=(VM, VM),
        scratch_shapes=[
            pltpu.VMEM((128, 1024), BF16),
            pltpu.VMEM((1024, 2048), BF16),
            pltpu.SemaphoreType.DMA((5,)),
        ],
        compiler_params=params(14),
        cost_estimate=cost(2 * 128 * 1024 * 2048 * 4, 6 << 20),
        name="conv_out",
    )(parts, w)


def attn_out_kernel(parts, conv, w, out, rows):
    for c in range(8):
        rows[:, 128 * c : 128 * c + 128] = parts[c]
    for j in range(4):
        cols = slice(512 * j, 512 * j + 512)
        out[:, cols] = (dot(rows[...], w[:, cols]) + conv[:, cols]).astype(BF16)


def attn_out(parts, conv, w):
    return pl.pallas_call(
        attn_out_kernel,
        out_shape=jax.ShapeDtypeStruct((128, 2048), BF16),
        in_specs=[VM, VM, VM],
        out_specs=VM,
        scratch_shapes=[pltpu.VMEM((128, 1024), BF16)],
        compiler_params=params(10),
        cost_estimate=cost(2 * 128 * 1024 * 2048 * 4, 6 << 20),
        name="attn_out",
    )(parts, conv, w)


def levels(*pairs):
    return [(a * SIDE + x, b * SIDE + x) for a, b in pairs for x in range(SIDE)]


def along_x(d):
    return [(z * SIDE + x, z * SIDE + (x + d) % SIDE) for z in (2, 3) for x in range(SIDE)]


def layer(x, wq, wk, wv, wu, wg, taps, gain, gate, w_out):
    x, wq, wk, wv, wu, wg, w_out = (
        pltpu.with_memory_space_constraint(v, pltpu.HBM) for v in (x, wq, wk, wv, wu, wg, w_out)
    )
    own = lax.axis_index("sp").astype(I32).reshape(1)
    table = jnp.asarray(work_table())
    pkv, pxx, pq, gated, tail = project(own, x, wq, wk, wv, wu, wg, gate.reshape(8, 128))
    halo = lax.ppermute(tail, "sp", [(i, i + 1) for i in range(15)])
    x1 = lax.ppermute(pxx, "sp", moves(-1, 0))
    x3 = lax.ppermute(pxx, "sp", moves(-3, 0))
    ky = lax.ppermute(pkv, "sp", levels((2, 3), (0, 2)))
    u = lax.ppermute(pq, "sp", levels((1, 0), (3, 1)))
    kz = lax.ppermute(pkv, "sp", levels((1, 2), (0, 3)))
    w = lax.ppermute(pq, "sp", levels((2, 1), (3, 0)))
    x2 = lax.ppermute(pxx, "sp", moves(-2, 0))
    conv = convolve(gated, halo, taps, gain.reshape(1, 128))
    conv_parts = lax.all_to_all(conv, "tp", 0, 0, tiled=True)
    *state, b1, b3 = attend_near(table, own, pkv, pq, x1, x3, u, w, kz, ky)
    back1 = lax.ppermute(b1, "sp", along_x(1))
    back3 = lax.ppermute(b3, "sp", along_x(3))
    o_own, lse_own, bu, b2 = attend_far(table, own, x2, state)
    back2 = lax.ppermute(b2, "sp", along_x(2))
    back_u = lax.ppermute(bu, "sp", levels((0, 1), (1, 3)))
    back_w = lax.ppermute(b2, "sp", levels((1, 2), (0, 3)))
    conv_mixed, w_attn = conv_out(conv_parts, w_out)
    mixed = combine(own, o_own, lse_own, (back1, back2, back3, back_u, back_w))
    attn_parts = lax.all_to_all(mixed, "tp", 0, 0, tiled=True)
    return attn_out(attn_parts, conv_mixed, w_attn)


def solution(mesh):
    in_specs = (
        P("sp", None),
        P(None, "tp"),
        P(None, "tp"),
        P(None, "tp"),
        P(None, "tp"),
        P(None, "tp"),
        P(None, "tp"),
        P("tp"),
        P("sp", "tp"),
        P(),
    )
    out_specs = P(("sp", "tp"), None)
    return jax.shard_map(layer, mesh=mesh, in_specs=in_specs, out_specs=out_specs, check_vma=False)
```

```python
import functools

import jax
import jax.numpy as jnp
import numpy as np
from jax import lax
from jax.experimental import pallas as pl
from jax.experimental.pallas import tpu as pltpu
from jax.sharding import PartitionSpec as P


BF16, F32, I32 = jnp.bfloat16, jnp.float32, jnp.int32
SIDE = 4
HEAD = 128
TOK = 1024
HALF = 512
TAPS = 31
GATE_ROW = TOK
PACK_ROWS = TOK + 16
BACK_ROWS = HALF + 16
TILES = 15
LOG2E = 1.4426950408889634
SCALE = HEAD**-0.5 * LOG2E
LOW = -1e30
TINY = 1e-37
EPS = 1e-05

VM = pl.BlockSpec(memory_space=pltpu.VMEM)
SM = pl.BlockSpec(memory_space=pltpu.SMEM)
ANY = pl.BlockSpec(memory_space=pl.ANY)
HBM = pl.BlockSpec(memory_space=pltpu.HBM)


def dot(a, b):
    return jnp.dot(a, b, preferred_element_type=F32)


def params(mib):
    return pltpu.CompilerParams(vmem_limit_bytes=mib << 20)


def cost(flops, moved):
    return pl.CostEstimate(flops=flops, bytes_accessed=moved, transcendentals=0)


def moves(dx, dz):
    return [
        (z * SIDE + x, (z + dz) % SIDE * SIDE + (x + dx) % SIDE)
        for z in range(SIDE)
        for x in range(SIDE)
    ]


def eye():
    return lax.broadcasted_iota(I32, (128, 128), 0) == lax.broadcasted_iota(I32, (128, 128), 1)


def to_row(column):
    return jnp.sum(jnp.where(eye(), column, 0.0), axis=0, keepdims=True)


def to_column(row):
    return jnp.sum(jnp.where(eye(), row, 0.0), axis=1, keepdims=True)


def split3(value):
    top = value.astype(BF16)
    rest = value - top.astype(F32)
    mid = rest.astype(BF16)
    return top, mid, (rest - mid.astype(F32)).astype(BF16)


UP_HALVES = np.array([[0, 0, 0, 1], [0, 0, 1, 2], [0, 1, 2, 2], [1, 2, 2, 2]])


def work_table():
    table = np.zeros((SIDE * SIDE, 3, TILES + 1), np.int32)
    for z in range(SIDE):
        for x in range(SIDE):
            tiles = []
            for d in range(SIDE):
                other = (x + d) % SIDE
                late = d == 2
                for h in range(2):
                    if z < 2:
                        tiles.append((True, 2 + h, d))
                        if other < x:
                            tiles.append((late, h, d))
                        if h < 2 - UP_HALVES[x, other]:
                            tiles.append((late, 4 + h, d))
                    else:
                        tiles.append((True, 2 * d + h, 2))
                        if other > x:
                            tiles.append((late, 2 * d + h, 0))
                        if h >= 2 - UP_HALVES[other, x]:
                            tiles.append((late, 2 * d + h, 1))
            near = sum(not t[0] for t in tiles)
            assert len(tiles) == TILES and near % 2 == 1
            for n, (_, q, k) in enumerate(sorted(tiles)):
                table[z * SIDE + x, :2, n] = q, k
            table[z * SIDE + x, 2, 0] = near
    return table


def gate_rows(both):
    return (both[:, :128] * jax.nn.sigmoid(both[:, 128:])).astype(BF16)


def project_kernel(
    own, x_hbm, wq, wk, wv, wu, wg, gate, pkv, pxx, pr, pq, gated, tail, x, w, sems
):
    low_level = own[0] < 8
    even_level = own[0] // SIDE % 2 == 0
    arrivals = [
        pltpu.make_async_copy(
            x_hbm.at[pl.ds(256 * i, 256)], x.at[pl.ds(256 * i, 256)], sems.at[i]
        )
        for i in range(4)
    ]
    loads = [
        pltpu.make_async_copy(source, w.at[:, pl.ds(128 * n, 128)], sems.at[4 + n])
        for n, source in enumerate((wk, wv, wq, wu, wg))
    ]
    for c in (*loads[:3], *arrivals, *loads[3:]):
        c.start()
    zero = jnp.zeros((8, 128), BF16)
    top, mid, low = split3(gate[...] * (-LOG2E))
    gates = jnp.concatenate(
        [jnp.concatenate([top, mid], axis=1), jnp.concatenate([low, zero], axis=1)], axis=0
    )
    pkv[GATE_ROW : GATE_ROW + 16, :] = gates
    pxx[GATE_ROW : GATE_ROW + 16, :] = gates
    pr[GATE_ROW : GATE_ROW + 16, :] = gates
    for c in loads[:3]:
        c.wait()
    for i in range(4):
        arrivals[i].wait()
        out = dot(x[256 * i : 256 * i + 256, :], w[:, :384])
        both = out[:, :256].astype(BF16)
        query = (out[:, 256:] * SCALE).astype(BF16)
        rows = slice(256 * i, 256 * i + 256)
        half = slice(256 * (i % 2), 256 * (i % 2) + 256)
        lanes = slice(128 * (i // 2), 128 * (i // 2) + 128)
        pkv[rows, :] = both
        pq[half, lanes] = query
        for pack, keys_go in ((pxx, low_level), (pr, even_level)):
            if i >= 2:
                pack[rows, :] = both
            else:

                @pl.when(keys_go)
                def _(pack=pack):
                    pack[rows, :] = both

            @pl.when(jnp.logical_not(keys_go))
            def _(pack=pack):
                pack[half, lanes] = query

    for c in loads[3:]:
        c.wait()
    for i in range(4):
        rows = gate_rows(dot(x[256 * i : 256 * i + 256, :], w[:, 384:]))
        gated[256 * i : 256 * i + 256, :] = rows
    tail[...] = rows[224:, :]


def project(own, x, wq, wk, wv, wu, wg, gate):
    pack = jax.ShapeDtypeStruct((PACK_ROWS, 256), BF16)
    return pl.pallas_call(
        project_kernel,
        out_shape=(
            pack,
            pack,
            pack,
            jax.ShapeDtypeStruct((HALF, 256), BF16),
            jax.ShapeDtypeStruct((TOK, 128), BF16),
            jax.ShapeDtypeStruct((32, 128), BF16),
        ),
        in_specs=[SM] + [HBM] * 6 + [VM],
        out_specs=(VM,) * 6,
        scratch_shapes=[
            pltpu.VMEM((TOK, 2048), BF16),
            pltpu.VMEM((2048, 640), BF16),
            pltpu.SemaphoreType.DMA((9,)),
        ],
        compiler_params=params(12),
        cost_estimate=cost(2 * TOK * 2048 * 640, 8 << 20),
        name="project",
    )(own, x, wq, wk, wv, wu, wg, gate)


def conv_kernel(gated, halo, taps, gain, out, padded):
    padded[0:32, :] = halo[...].astype(F32)
    padded[32 : 32 + TOK, :] = gated[...].astype(F32)
    padded[32 + TOK :, :] = jnp.zeros((8, 128), F32)
    for block in range(8):
        start = 128 * block
        total = None
        for r in range(8):
            part = None
            for q in range(5):
                j = 8 * q + r - 2
                if 0 <= j < TAPS:
                    term = taps[j : j + 1, :] * padded[start + 8 * q : start + 8 * q + 136, :]
                    part = term if part is None else part + term
            part = part[r : r + 128, :]
            total = part if total is None else total + part
        out[block, 0:128, :] = total
        out[block, 128:136, :] = jnp.broadcast_to(gain[...], (8, 128))


def convolve(gated, halo, taps, gain):
    return pl.pallas_call(
        conv_kernel,
        out_shape=jax.ShapeDtypeStruct((8, 136, 128), F32),
        in_specs=[VM] * 4,
        out_specs=VM,
        scratch_shapes=[pltpu.VMEM((TOK + 40, 128), F32)],
        compiler_params=params(8),
        cost_estimate=cost(2 * TOK * 128 * 31 * 64, 1 << 20),
        name="convolve",
    )(gated, halo, taps, gain)


def diagonal(pkv, pq, m, l, acc):
    top = pkv[GATE_ROW : GATE_ROW + 8, :].astype(F32)
    low = pkv[GATE_ROW + 8 : GATE_ROW + 16, :].astype(F32)
    gates = top[:, :128] + top[:, 128:] + low[:, :128]
    for half in range(2):
        keys = HALF * (half + 1)
        scores = lax.dot_general(
            pq[:, 128 * half : 128 * half + 128],
            pkv[:keys, :128],
            (((1,), (1,)), ((), ())),
            preferred_element_type=F32,
        )
        row = lax.broadcasted_iota(I32, (HALF, 128), 0) + HALF * half
        lane = lax.broadcasted_iota(I32, (HALF, 128), 1)
        parts = []
        for c in range(keys // 128):
            t = scores[:, 128 * c : 128 * c + 128] + gates[c : c + 1, :]
            parts.append(jnp.where(lane + 128 * c <= row, t, LOW))
        most = functools.reduce(jnp.maximum, parts)
        most = jnp.broadcast_to(jnp.max(most, axis=1, keepdims=True), (HALF, 128))
        weights = [jnp.exp2(t - most) for t in parts]
        m[half] = most
        rounded = jnp.concatenate([w.astype(BF16) for w in weights], axis=1)
        ones = jnp.ones((keys, 128), BF16)
        out = dot(rounded, jnp.concatenate([pkv[:keys, 128:], ones], axis=1))
        acc[half] = out[:, :128]
        l[half] = out[:, 128:]


QUERIES = 8


def key_copies(source, packs, slot, sems):
    return [
        pltpu.make_async_copy(
            source.at[pl.ds(at, rows)], packs.at[slot, pl.ds(at, rows)], sems.at[n, slot]
        )
        for n, (at, rows) in enumerate(((0, HALF), (HALF, PACK_ROWS - HALF)))
    ]


def query_copy(source, qpacks, slot, sems):
    return pltpu.make_async_copy(source.at[pl.ds(0, HALF)], qpacks.at[slot], sems.at[2, slot])


def unpack_keys(packs, slots, gates):
    for n in slots:
        top = packs[n, GATE_ROW : GATE_ROW + 8, :].astype(F32)
        low = packs[n, GATE_ROW + 8 : GATE_ROW + 16, :].astype(F32)
        gates[n] = top[:, :128] + top[:, 128:] + low[:, :128]


def unpack_queries(qpacks, slots, query):
    for n in slots:
        query[2 * n] = qpacks[n, :, :128]
        query[2 * n + 1] = qpacks[n, :, 128:]


def each(copies, action):
    for c in copies:
        getattr(c, action)()


def finish(m, l, acc, first, out):
    for n in range(2):
        total = jnp.maximum(l[first + n], TINY)
        lse = m[first + n] + jnp.log2(total)
        base = BACK_ROWS * n
        out[base : base + HALF, :] = (acc[first + n] / total).astype(BF16)
        rows = [to_row(lse[128 * b : 128 * b + 128, :]) for b in range(4)]
        parts = split3(jnp.concatenate(rows + rows, axis=0))
        out[base + HALF : base + BACK_ROWS, :] = jnp.concatenate(
            [parts[0][:4], parts[1][:4], parts[2]], axis=0
        )


def run_tiles(table, own, start, count, even, packs, query, gates, per_tile, m, l, acc):
    sa, sb, ma, mb, aa, ab = per_tile
    row = own[0]
    first, second = (sa, ma, aa), (sb, mb, ab)

    def scores_of(n, s, most, shrink):
        q, k = table[row, 0, n], table[row, 1, n]
        raw = lax.dot_general(
            query[q], packs[k, :TOK, :128], (((1,), (1,)), ((), ())), preferred_element_type=F32
        )
        best = None
        for c in range(8):
            t = raw[:, 128 * c : 128 * c + 128] + gates[k, c : c + 1, :]
            s[:, 128 * c : 128 * c + 128] = t
            best = t if best is None else jnp.maximum(best, t)
        old = m[q]
        new = jnp.maximum(old, jnp.max(best, axis=1, keepdims=True))
        shrink[...] = jnp.exp2(old - new)
        m[q] = new
        most[...] = new

    def weigh(n, s, most, shrink):
        q, k = table[row, 0, n], table[row, 1, n]
        top = most[...]
        by = shrink[...]
        w = [jnp.exp2(s[:, 128 * c : 128 * c + 128] - top) for c in range(8)]
        rounded = jnp.concatenate([v.astype(BF16) for v in w], axis=1)
        ones = jnp.ones((TOK, 128), BF16)
        out = dot(rounded, jnp.concatenate([packs[k, :TOK, 128:], ones], axis=1))
        acc[q] = acc[q] * by + out[:, :128]
        l[q] = l[q] * by + out[:, 128:]


    scores_of(start, *first)

    def two_tiles(i, carry):
        n = start + 2 * i
        scores_of(n + 1, *second)
        weigh(n, *first)
        scores_of(n + 2, *first)
        weigh(n + 1, *second)
        return carry

    lax.fori_loop(0, (count - 1) // 2, two_tiles, 0)
    if even:
        scores_of(start + count - 1, *second)
        weigh(start + count - 2, *first)
        weigh(start + count - 1, *second)
    else:
        weigh(start + count - 1, *first)


def by_level(own, low_job, high_job):
    pl.when(own[0] < 8)(low_job)
    pl.when(own[0] >= 8)(high_job)


def near_kernel(
    table, own, pkv, pq, x1, x3, swapped,
    m, l, acc, packs, query, gates, qpacks, sems, *per_tile,
):
    own_copies = [*key_copies(pkv, packs, 0, sems), query_copy(pq, qpacks, 0, sems)]
    low_copies = [
        *key_copies(x1, packs, 1, sems),
        *key_copies(x3, packs, 3, sems),
        query_copy(swapped, qpacks, 2, sems),
    ]
    high_copies = [
        *key_copies(swapped, packs, 1, sems),
        query_copy(x1, qpacks, 1, sems),
        query_copy(x3, qpacks, 3, sems),
    ]
    each(own_copies, "start")
    by_level(own, lambda: each(low_copies, "start"), lambda: each(high_copies, "start"))
    for n in range(2, QUERIES):
        m[n] = jnp.full((HALF, 128), LOW, F32)
        l[n] = jnp.zeros((HALF, 128), F32)
        acc[n] = jnp.zeros((HALF, 128), F32)
    each(own_copies, "wait")
    unpack_keys(packs, (0,), gates)
    unpack_queries(qpacks, (0,), query)
    diagonal(packs.at[0], qpacks.at[0], m, l, acc)

    def low_job():
        each(low_copies, "wait")
        unpack_keys(packs, (1, 3), gates)
        unpack_queries(qpacks, (2,), query)

    def high_job():
        each(high_copies, "wait")
        unpack_keys(packs, (1,), gates)
        unpack_queries(qpacks, (1, 3), query)

    by_level(own, low_job, high_job)
    count = table[own[0], 2, 0]
    run_tiles(table, own, 0, count, False, packs, query, gates, per_tile, m, l, acc)


def far_kernel(
    table, own, x2, turned, m_in, l_in, acc_in, packs_in, query_in, gates_in,
    o_own, lse_own, b1, b2, b3,
    m, l, acc, packs, query, gates, qpacks, sems, *per_tile,
):
    low_copies = [*key_copies(x2, packs, 2, sems), query_copy(turned, qpacks, 1, sems)]
    high_copies = [*key_copies(turned, packs, 2, sems), query_copy(x2, qpacks, 2, sems)]
    by_level(own, lambda: each(low_copies, "start"), lambda: each(high_copies, "start"))
    for n in range(QUERIES):
        m[n] = m_in[n]
        l[n] = l_in[n]
        acc[n] = acc_in[n]
        query[n] = query_in[n]
    for n in (0, 1, 3):
        packs[n, :TOK, :] = packs_in[n, :TOK, :]
        gates[n] = gates_in[n]

    def low_job():
        each(low_copies, "wait")
        unpack_queries(qpacks, (1,), query)

    def high_job():
        each(high_copies, "wait")
        unpack_queries(qpacks, (2,), query)

    by_level(own, low_job, high_job)
    unpack_keys(packs, (2,), gates)
    near = table[own[0], 2, 0]
    run_tiles(table, own, near, TILES - near, True, packs, query, gates, per_tile, m, l, acc)
    for n in range(2):
        total = jnp.maximum(l[n], TINY)
        o_own[n] = acc[n] / total
        lse_own[n] = m[n] + jnp.log2(total)
    for n, back in enumerate((b1, b2, b3)):
        finish(m, l, acc, 2 * n + 2, back)


SEMS = [pltpu.SemaphoreType.DMA((3, 4))]
QPACKS = [((4, HALF, 256), BF16)]
SLOTS = [((4, PACK_ROWS, 256), BF16), ((QUERIES, HALF, 128), BF16), ((4, 8, 128), F32)]
STATE = [((QUERIES, HALF, 128), F32)] * 3
TILE = [((HALF, TOK), F32)] * 2 + [((HALF, 128), F32)] * 4
BACK = [((2 * BACK_ROWS, 128), BF16)]


def arrays(shapes):
    return tuple(jax.ShapeDtypeStruct(*v) for v in shapes)


def scratch(shapes):
    return [pltpu.VMEM(*v) for v in shapes]


def attend_near(table, own, *packs):
    return pl.pallas_call(
        near_kernel,
        out_shape=arrays(STATE + SLOTS),
        in_specs=[SM, SM] + [ANY] * 5,
        out_specs=(VM,) * 6,
        scratch_shapes=scratch(QPACKS) + SEMS + scratch(TILE),
        compiler_params=params(24),
        cost_estimate=cost(6 * 4 * HALF * TOK * 256, 8 << 20),
        name="attend_near",
    )(table, own, *packs)


def attend_far(table, own, x2, turned, state):
    return pl.pallas_call(
        far_kernel,
        out_shape=arrays([((2, HALF, 128), F32)] * 2 + BACK * 3),
        in_specs=[SM, SM, ANY, ANY] + [VM] * 6,
        out_specs=(VM,) * 5,
        scratch_shapes=scratch(STATE + SLOTS + QPACKS) + SEMS + scratch(TILE),
        compiler_params=params(30),
        cost_estimate=cost(10 * 4 * HALF * TOK * 256, 8 << 20),
        name="attend_far",
    )(table, own, x2, turned, *state)


def combine_kernel(own, o_own, lse_own, x1, x2, x3, u, w, out):
    z = own[0] // SIDE
    high = z >= 2
    backs = ((x1, high), (x2, high), (x3, high), (u, z % 2 == 1), (w, high))
    for half in range(2):
        base = BACK_ROWS * half
        lses = []
        for back, there in backs:
            tail = back[base + HALF : base + BACK_ROWS, :].astype(F32)
            lses.append(jnp.where(there, tail[0:4] + tail[4:8] + tail[8:12], LOW))
        for b in range(4):
            rows = slice(128 * b, 128 * b + 128)
            columns = [lse_own[half, rows, :]]
            columns += [jnp.broadcast_to(to_column(v[b : b + 1, :]), (128, 128)) for v in lses]
            most = functools.reduce(jnp.maximum, columns)
            shares = [jnp.exp2(c - most) for c in columns]
            mixed = shares[0] * o_own[half, rows, :]
            for share, (back, _) in zip(shares[1:], backs):
                mixed = mixed + share * back[base + 128 * b : base + 128 * b + 128, :].astype(F32)
            out[4 * half + b] = (mixed / functools.reduce(jnp.add, shares)).astype(BF16)


def combine(own, o_own, lse_own, backs):
    return pl.pallas_call(
        combine_kernel,
        out_shape=jax.ShapeDtypeStruct((8, 128, 128), BF16),
        in_specs=[SM] + [VM] * 7,
        out_specs=VM,
        compiler_params=params(16),
        cost_estimate=cost(1 << 29, 2 << 20),
        name="combine",
    )(own, o_own, lse_own, *backs)


def conv_out_kernel(parts, w_hbm, out, later, rows, w, sems):
    copies = []
    for j in range(4):
        cols = pl.ds(512 * j, 512)
        copies.append(
            pltpu.make_async_copy(w_hbm.at[pl.ds(0, 1024), cols], w.at[:, cols], sems.at[j])
        )
    copies.append(pltpu.make_async_copy(w_hbm.at[pl.ds(1024, 1024)], later, sems.at[4]))
    for c in copies:
        c.start()
    total = functools.reduce(jnp.add, [parts[c, :128, :] for c in range(8)])
    mean = jnp.sum(total, axis=1, keepdims=True) * (1.0 / 1024)
    far = [parts[c, :128, :] - mean for c in range(8)]
    spread = functools.reduce(jnp.add, [v * v for v in far])
    spread = jnp.sum(spread, axis=1, keepdims=True) * (1.0 / 1024)
    inverse = lax.rsqrt(spread + EPS)
    for c in range(8):
        v = far[c] * inverse * parts[c, 128:129, :]
        rows[:, 128 * c : 128 * c + 128] = (v * jax.nn.sigmoid(v)).astype(BF16)
    for j in range(4):
        copies[j].wait()
        out[:, 512 * j : 512 * j + 512] = dot(rows[...], w[:, 512 * j : 512 * j + 512])
    copies[4].wait()


def conv_out(parts, w):
    return pl.pallas_call(
        conv_out_kernel,
        out_shape=(
            jax.ShapeDtypeStruct((128, 2048), F32),
            jax.ShapeDtypeStruct((1024, 2048), BF16),
        ),
        in_specs=[VM, HBM],
        out_specs=(VM, VM),
        scratch_shapes=[
            pltpu.VMEM((128, 1024), BF16),
            pltpu.VMEM((1024, 2048), BF16),
            pltpu.SemaphoreType.DMA((5,)),
        ],
        compiler_params=params(14),
        cost_estimate=cost(2 * 128 * 1024 * 2048 * 4, 6 << 20),
        name="conv_out",
    )(parts, w)


def attn_out_kernel(parts, conv, w, out, rows):
    for c in range(8):
        rows[:, 128 * c : 128 * c + 128] = parts[c]
    for j in range(4):
        cols = slice(512 * j, 512 * j + 512)
        out[:, cols] = (dot(rows[...], w[:, cols]) + conv[:, cols]).astype(BF16)


def attn_out(parts, conv, w):
    return pl.pallas_call(
        attn_out_kernel,
        out_shape=jax.ShapeDtypeStruct((128, 2048), BF16),
        in_specs=[VM, VM, VM],
        out_specs=VM,
        scratch_shapes=[pltpu.VMEM((128, 1024), BF16)],
        compiler_params=params(10),
        cost_estimate=cost(2 * 128 * 1024 * 2048 * 4, 6 << 20),
        name="attn_out",
    )(parts, conv, w)


def levels(*pairs):
    return [(a * SIDE + x, b * SIDE + x) for a, b in pairs for x in range(SIDE)]


def along_x(d):
    return [(z * SIDE + x, z * SIDE + (x + d) % SIDE) for z in (2, 3) for x in range(SIDE)]


def layer(x, wq, wk, wv, wu, wg, taps, gain, gate, w_out):
    x, wq, wk, wv, wu, wg, w_out = (
        pltpu.with_memory_space_constraint(v, pltpu.HBM) for v in (x, wq, wk, wv, wu, wg, w_out)
    )
    own = lax.axis_index("sp").astype(I32).reshape(1)
    table = jnp.asarray(work_table())
    pkv, pxx, pr, pq, gated, tail = project(own, x, wq, wk, wv, wu, wg, gate.reshape(8, 128))
    halo = lax.ppermute(tail, "sp", [(i, i + 1) for i in range(15)])
    x1 = lax.ppermute(pxx, "sp", moves(-1, 0))
    x3 = lax.ppermute(pxx, "sp", moves(-3, 0))
    turned = lax.ppermute(pr, "sp", levels((0, 2), (2, 3), (3, 1), (1, 0)))
    swapped = lax.ppermute(pxx, "sp", levels((0, 3), (1, 2), (2, 1), (3, 0)))
    x2 = lax.ppermute(pxx, "sp", moves(-2, 0))
    conv = convolve(gated, halo, taps, gain.reshape(1, 128))
    conv_parts = lax.all_to_all(conv, "tp", 0, 0, tiled=True)
    near = (in_hbm(pkv), in_hbm(pq), x1, x3, swapped)
    state = attend_near(table, own, *near)
    far = attend_far(table, own, x2, turned, state)
    o_own, lse_own, b1, b2, b3 = far
    back1 = lax.ppermute(b1, "sp", along_x(1))
    back3 = lax.ppermute(b3, "sp", along_x(3))
    back2 = lax.ppermute(b2, "sp", along_x(2))
    back_u = lax.ppermute(b1, "sp", levels((0, 1), (1, 3)))
    back_w = lax.ppermute(b2, "sp", levels((1, 2), (0, 3)))
    conv_mixed, w_attn = conv_out(conv_parts, w_out)
    mixed = combine(own, o_own, lse_own, (back1, back2, back3, back_u, back_w))
    attn_parts = lax.all_to_all(mixed, "tp", 0, 0, tiled=True)
    return attn_out(attn_parts, conv_mixed, w_attn)


def in_hbm(value):
    return pltpu.with_memory_space_constraint(value, pltpu.HBM)


def solution(mesh):
    in_specs = (
        P("sp", None),
        P(None, "tp"),
        P(None, "tp"),
        P(None, "tp"),
        P(None, "tp"),
        P(None, "tp"),
        P(None, "tp"),
        P("tp"),
        P("sp", "tp"),
        P(),
    )
    out_specs = P(("sp", "tp"), None)
    return jax.shard_map(layer, mesh=mesh, in_specs=in_specs, out_specs=out_specs, check_vma=False)
```

```python
import functools

import jax
import jax.numpy as jnp
import numpy as np
from jax import lax
from jax.experimental import pallas as pl
from jax.experimental.pallas import tpu as pltpu
from jax.sharding import PartitionSpec as P


BF16, F32, I32 = jnp.bfloat16, jnp.float32, jnp.int32
SIDE = 4
HEAD = 128
TOK = 1024
HALF = 512
TAPS = 31
GATE_ROW = TOK
PACK_ROWS = TOK + 16
BACK_ROWS = HALF + 16
TILES = 17
LOG2E = 1.4426950408889634
SCALE = HEAD**-0.5 * LOG2E
LOW = -1e30
TINY = 1e-37
EPS = 1e-05

VM = pl.BlockSpec(memory_space=pltpu.VMEM)
SM = pl.BlockSpec(memory_space=pltpu.SMEM)
ANY = pl.BlockSpec(memory_space=pl.ANY)
HBM = pl.BlockSpec(memory_space=pltpu.HBM)


def dot(a, b):
    return jnp.dot(a, b, preferred_element_type=F32)


def params(mib):
    return pltpu.CompilerParams(vmem_limit_bytes=mib << 20)


def cost(flops, moved):
    return pl.CostEstimate(flops=flops, bytes_accessed=moved, transcendentals=0)


def moves(dx, dz):
    return [
        (z * SIDE + x, (z + dz) % SIDE * SIDE + (x + dx) % SIDE)
        for z in range(SIDE)
        for x in range(SIDE)
    ]


def eye():
    return lax.broadcasted_iota(I32, (128, 128), 0) == lax.broadcasted_iota(I32, (128, 128), 1)


def to_row(column):
    return jnp.sum(jnp.where(eye(), column, 0.0), axis=0, keepdims=True)


def to_column(row):
    return jnp.sum(jnp.where(eye(), row, 0.0), axis=1, keepdims=True)


def split3(value):
    top = value.astype(BF16)
    rest = value - top.astype(F32)
    mid = rest.astype(BF16)
    return top, mid, (rest - mid.astype(F32)).astype(BF16)


UP_HALVES = np.array([[0, 0, 0, 1], [0, 0, 1, 0], [0, 1, 0, 2], [1, 0, 2, 2]])


def work_table():
    table = np.zeros((SIDE * SIDE, 3, TILES + 1), np.int32)
    for z in range(SIDE):
        for x in range(SIDE):
            tiles = []
            for d in range(SIDE):
                other = (x + d) % SIDE
                late = d == 2
                for h in range(2):
                    if z < 2:
                        tiles.append((True, 2 + h, d))
                        if other < x:
                            tiles.append((late, h, d))
                        if h < 2 - UP_HALVES[x, other]:
                            tiles.append((late, 4 + h, d))
                    else:
                        tiles.append((True, 2 * d + h, 2))
                        if other > x:
                            tiles.append((late, 2 * d + h, 0))
                        if h >= 2 - UP_HALVES[other, x]:
                            tiles.append((late, 2 * d + h, 1))
            near = sum(not t[0] for t in tiles)
            assert len(tiles) <= TILES and len(tiles) % 2 == 1 and near % 2 == 1
            for n, (_, q, k) in enumerate(sorted(tiles)):
                table[z * SIDE + x, :2, n] = q, k
            table[z * SIDE + x, 2, :2] = near, len(tiles)
    return table


def gate_rows(both):
    return (both[:, :128] * jax.nn.sigmoid(both[:, 128:])).astype(BF16)


def project_kernel(
    own, x_hbm, wq, wk, wv, wu, wg, gate_hbm, pkv_hbm, pxx, pr, pq_hbm, gated, tail,
    x, w, pkv, pq, gate, sems,
):
    low_level = own[0] < 8
    even_level = own[0] // SIDE % 2 == 0
    arrivals = [
        pltpu.make_async_copy(
            x_hbm.at[pl.ds(256 * i, 256)], x.at[pl.ds(256 * i, 256)], sems.at[i]
        )
        for i in range(4)
    ]
    loads = [
        pltpu.make_async_copy(source, w.at[:, pl.ds(128 * n, 128)], sems.at[4 + n])
        for n, source in enumerate((wk, wv, wq, wu, wg))
    ]
    gate_load = pltpu.make_async_copy(gate_hbm, gate, sems.at[9])
    for c in (gate_load, *loads[:3], *arrivals, *loads[3:]):
        c.start()
    gate_load.wait()
    zero = jnp.zeros((8, 128), BF16)
    top, mid, low = split3(gate[...] * (-LOG2E))
    gates = jnp.concatenate(
        [jnp.concatenate([top, mid], axis=1), jnp.concatenate([low, zero], axis=1)], axis=0
    )
    pkv[GATE_ROW : GATE_ROW + 16, :] = gates
    pxx[GATE_ROW : GATE_ROW + 16, :] = gates
    pr[GATE_ROW : GATE_ROW + 16, :] = gates
    for c in loads[:3]:
        c.wait()
    for i in range(4):
        arrivals[i].wait()
        out = dot(x[256 * i : 256 * i + 256, :], w[:, :384])
        both = out[:, :256].astype(BF16)
        query = (out[:, 256:] * SCALE).astype(BF16)
        rows = slice(256 * i, 256 * i + 256)
        half = slice(256 * (i % 2), 256 * (i % 2) + 256)
        lanes = slice(128 * (i // 2), 128 * (i // 2) + 128)
        pkv[rows, :] = both
        pq[half, lanes] = query
        for pack, keys_go in ((pxx, low_level), (pr, even_level)):
            if i >= 2:
                pack[rows, :] = both
            else:

                @pl.when(keys_go)
                def _(pack=pack):
                    pack[rows, :] = both

            @pl.when(jnp.logical_not(keys_go))
            def _(pack=pack):
                pack[half, lanes] = query

    keeps = [
        pltpu.make_async_copy(pkv, pkv_hbm, sems.at[10]),
        pltpu.make_async_copy(pq, pq_hbm, sems.at[11]),
    ]
    for c in keeps:
        c.start()
    for c in loads[3:]:
        c.wait()
    for i in range(4):
        rows = gate_rows(dot(x[256 * i : 256 * i + 256, :], w[:, 384:]))
        gated[256 * i : 256 * i + 256, :] = rows
    tail[...] = rows[224:, :]
    for c in keeps:
        c.wait()


def project(own, x, wq, wk, wv, wu, wg, gate):
    pack = jax.ShapeDtypeStruct((PACK_ROWS, 256), BF16)
    return pl.pallas_call(
        project_kernel,
        out_shape=(
            pltpu.HBM((PACK_ROWS, 256), BF16),
            pack,
            pack,
            pltpu.HBM((HALF, 256), BF16),
            jax.ShapeDtypeStruct((TOK, 128), BF16),
            jax.ShapeDtypeStruct((32, 128), BF16),
        ),
        in_specs=[SM] + [HBM] * 7,
        out_specs=(HBM, VM, VM, HBM, VM, VM),
        scratch_shapes=[
            pltpu.VMEM((TOK, 2048), BF16),
            pltpu.VMEM((2048, 640), BF16),
            pltpu.VMEM((PACK_ROWS, 256), BF16),
            pltpu.VMEM((HALF, 256), BF16),
            pltpu.VMEM((8, 128), F32),
            pltpu.SemaphoreType.DMA((12,)),
        ],
        compiler_params=params(12),
        cost_estimate=cost(2 * TOK * 2048 * 640, 8 << 20),
        name="project",
    )(own, x, wq, wk, wv, wu, wg, gate)


def conv_kernel(gated, halo, taps, gain, out, padded):
    padded[0:32, :] = halo[...].astype(F32)
    padded[32 : 32 + TOK, :] = gated[...].astype(F32)
    padded[32 + TOK :, :] = jnp.zeros((8, 128), F32)
    for block in range(8):
        start = 128 * block
        total = None
        for r in range(8):
            part = None
            for q in range(5):
                j = 8 * q + r - 2
                if 0 <= j < TAPS:
                    term = taps[j : j + 1, :] * padded[start + 8 * q : start + 8 * q + 136, :]
                    part = term if part is None else part + term
            part = part[r : r + 128, :]
            total = part if total is None else total + part
        out[block, 0:128, :] = total
        out[block, 128:136, :] = jnp.broadcast_to(gain[...], (8, 128))


def convolve(gated, halo, taps, gain):
    return pl.pallas_call(
        conv_kernel,
        out_shape=jax.ShapeDtypeStruct((8, 136, 128), F32),
        in_specs=[VM] * 4,
        out_specs=VM,
        scratch_shapes=[pltpu.VMEM((TOK + 40, 128), F32)],
        compiler_params=params(8),
        cost_estimate=cost(2 * TOK * 128 * 31 * 64, 1 << 20),
        name="convolve",
    )(gated, halo, taps, gain)


def diagonal(pkv, pq, m, l, acc):
    top = pkv[GATE_ROW : GATE_ROW + 8, :].astype(F32)
    low = pkv[GATE_ROW + 8 : GATE_ROW + 16, :].astype(F32)
    gates = top[:, :128] + top[:, 128:] + low[:, :128]
    for half in range(2):
        keys = HALF * (half + 1)
        scores = lax.dot_general(
            pq[:, 128 * half : 128 * half + 128],
            pkv[:keys, :128],
            (((1,), (1,)), ((), ())),
            preferred_element_type=F32,
        )
        row = lax.broadcasted_iota(I32, (HALF, 128), 0) + HALF * half
        lane = lax.broadcasted_iota(I32, (HALF, 128), 1)
        parts = []
        for c in range(keys // 128):
            t = scores[:, 128 * c : 128 * c + 128] + gates[c : c + 1, :]
            parts.append(jnp.where(lane + 128 * c <= row, t, LOW))
        most = functools.reduce(jnp.maximum, parts)
        most = jnp.broadcast_to(jnp.max(most, axis=1, keepdims=True), (HALF, 128))
        weights = [jnp.exp2(t - most) for t in parts]
        m[half] = most
        rounded = jnp.concatenate([w.astype(BF16) for w in weights], axis=1)
        ones = jnp.ones((keys, 128), BF16)
        out = dot(rounded, jnp.concatenate([pkv[:keys, 128:], ones], axis=1))
        acc[half] = out[:, :128]
        l[half] = out[:, 128:]


QUERIES = 8


def key_copies(source, packs, slot, sems):
    return [
        pltpu.make_async_copy(
            source.at[pl.ds(at, rows)], packs.at[slot, pl.ds(at, rows)], sems.at[n, slot]
        )
        for n, (at, rows) in enumerate(((0, HALF), (HALF, PACK_ROWS - HALF)))
    ]


def query_copy(source, qpacks, slot, sems):
    return pltpu.make_async_copy(source.at[pl.ds(0, HALF)], qpacks.at[slot], sems.at[2, slot])


def unpack_keys(packs, slots, gates):
    for n in slots:
        top = packs[n, GATE_ROW : GATE_ROW + 8, :].astype(F32)
        low = packs[n, GATE_ROW + 8 : GATE_ROW + 16, :].astype(F32)
        gates[n] = top[:, :128] + top[:, 128:] + low[:, :128]


def unpack_queries(qpacks, slots, query):
    for n in slots:
        query[2 * n] = qpacks[n, :, :128]
        query[2 * n + 1] = qpacks[n, :, 128:]


def each(copies, action):
    for c in copies:
        getattr(c, action)()


def finish(m, l, acc, first, out):
    for n in range(2):
        total = jnp.maximum(l[first + n], TINY)
        lse = m[first + n] + jnp.log2(total)
        base = BACK_ROWS * n
        out[base : base + HALF, :] = (acc[first + n] / total).astype(BF16)
        rows = [to_row(lse[128 * b : 128 * b + 128, :]) for b in range(4)]
        parts = split3(jnp.concatenate(rows + rows, axis=0))
        out[base + HALF : base + BACK_ROWS, :] = jnp.concatenate(
            [parts[0][:4], parts[1][:4], parts[2]], axis=0
        )


def run_tiles(table, own, start, count, even, packs, query, gates, per_tile, m, l, acc):
    sa, sb, ma, mb, aa, ab = per_tile
    row = own[0]
    first, second = (sa, ma, aa), (sb, mb, ab)

    def scores_of(n, s, most, shrink):
        q, k = table[row, 0, n], table[row, 1, n]
        raw = lax.dot_general(
            query[q], packs[k, :TOK, :128], (((1,), (1,)), ((), ())), preferred_element_type=F32
        )
        best = None
        for c in range(8):
            t = raw[:, 128 * c : 128 * c + 128] + gates[k, c : c + 1, :]
            s[:, 128 * c : 128 * c + 128] = t
            best = t if best is None else jnp.maximum(best, t)
        old = m[q]
        new = jnp.maximum(old, jnp.max(best, axis=1, keepdims=True))
        shrink[...] = jnp.exp2(old - new)
        m[q] = new
        most[...] = new

    def weigh(n, s, most, shrink):
        q, k = table[row, 0, n], table[row, 1, n]
        top = most[...]
        by = shrink[...]
        w = [jnp.exp2(s[:, 128 * c : 128 * c + 128] - top) for c in range(8)]
        rounded = jnp.concatenate([v.astype(BF16) for v in w], axis=1)
        ones = jnp.ones((TOK, 128), BF16)
        out = dot(rounded, jnp.concatenate([packs[k, :TOK, 128:], ones], axis=1))
        acc[q] = acc[q] * by + out[:, :128]
        l[q] = l[q] * by + out[:, 128:]


    scores_of(start, *first)

    def two_tiles(i, carry):
        n = start + 2 * i
        scores_of(n + 1, *second)
        weigh(n, *first)
        scores_of(n + 2, *first)
        weigh(n + 1, *second)
        return carry

    lax.fori_loop(0, (count - 1) // 2, two_tiles, 0)
    if even:
        scores_of(start + count - 1, *second)
        weigh(start + count - 2, *first)
        weigh(start + count - 1, *second)
    else:
        weigh(start + count - 1, *first)


def by_level(own, low_job, high_job):
    pl.when(own[0] < 8)(low_job)
    pl.when(own[0] >= 8)(high_job)


def near_kernel(
    table, own, pkv, pq, x1, x3, swapped,
    m, l, acc, packs, query, gates, qpacks, sems, *per_tile,
):
    own_copies = [*key_copies(pkv, packs, 0, sems), query_copy(pq, qpacks, 0, sems)]
    low_copies = [
        *key_copies(x1, packs, 1, sems),
        *key_copies(x3, packs, 3, sems),
        query_copy(swapped, qpacks, 2, sems),
    ]
    high_copies = [
        *key_copies(swapped, packs, 1, sems),
        query_copy(x1, qpacks, 1, sems),
        query_copy(x3, qpacks, 3, sems),
    ]
    each(own_copies, "start")
    by_level(own, lambda: each(low_copies, "start"), lambda: each(high_copies, "start"))
    for n in range(2, QUERIES):
        m[n] = jnp.full((HALF, 128), LOW, F32)
        l[n] = jnp.zeros((HALF, 128), F32)
        acc[n] = jnp.zeros((HALF, 128), F32)
    each(own_copies, "wait")
    unpack_keys(packs, (0,), gates)
    unpack_queries(qpacks, (0,), query)
    diagonal(packs.at[0], qpacks.at[0], m, l, acc)

    def low_job():
        each(low_copies, "wait")
        unpack_keys(packs, (1, 3), gates)
        unpack_queries(qpacks, (2,), query)

    def high_job():
        each(high_copies, "wait")
        unpack_keys(packs, (1,), gates)
        unpack_queries(qpacks, (1, 3), query)

    by_level(own, low_job, high_job)
    count = table[own[0], 2, 0]
    run_tiles(table, own, 0, count, False, packs, query, gates, per_tile, m, l, acc)


def far_kernel(
    table, own, x2, turned, m_in, l_in, acc_in, packs_in, query_in, gates_in,
    o_own, lse_own, b1, b2, b3,
    m, l, acc, packs, query, gates, qpacks, sems, *per_tile,
):
    low_copies = [*key_copies(x2, packs, 2, sems), query_copy(turned, qpacks, 1, sems)]
    high_copies = [*key_copies(turned, packs, 2, sems), query_copy(x2, qpacks, 2, sems)]
    by_level(own, lambda: each(low_copies, "start"), lambda: each(high_copies, "start"))
    for n in range(QUERIES):
        m[n] = m_in[n]
        l[n] = l_in[n]
        acc[n] = acc_in[n]
        query[n] = query_in[n]
    for n in (0, 1, 3):
        packs[n, :TOK, :] = packs_in[n, :TOK, :]
        gates[n] = gates_in[n]

    def low_job():
        each(low_copies, "wait")
        unpack_queries(qpacks, (1,), query)

    def high_job():
        each(high_copies, "wait")
        unpack_queries(qpacks, (2,), query)

    by_level(own, low_job, high_job)
    unpack_keys(packs, (2,), gates)
    near = table[own[0], 2, 0]
    run_tiles(table, own, near, table[own[0], 2, 1] - near, True, packs, query, gates, per_tile, m, l, acc)
    for n in range(2):
        total = jnp.maximum(l[n], TINY)
        o_own[n] = acc[n] / total
        lse_own[n] = m[n] + jnp.log2(total)
    for n, back in enumerate((b1, b2, b3)):
        finish(m, l, acc, 2 * n + 2, back)


SEMS = [pltpu.SemaphoreType.DMA((3, 4))]
QPACKS = [((4, HALF, 256), BF16)]
SLOTS = [((4, PACK_ROWS, 256), BF16), ((QUERIES, HALF, 128), BF16), ((4, 8, 128), F32)]
STATE = [((QUERIES, HALF, 128), F32)] * 3
TILE = [((HALF, TOK), F32)] * 2 + [((HALF, 128), F32)] * 4
BACK = [((2 * BACK_ROWS, 128), BF16)]


def arrays(shapes):
    return tuple(jax.ShapeDtypeStruct(*v) for v in shapes)


def scratch(shapes):
    return [pltpu.VMEM(*v) for v in shapes]


def attend_near(table, own, *packs):
    return pl.pallas_call(
        near_kernel,
        out_shape=arrays(STATE + SLOTS),
        in_specs=[SM, SM] + [ANY] * 5,
        out_specs=(VM,) * 6,
        scratch_shapes=scratch(QPACKS) + SEMS + scratch(TILE),
        compiler_params=params(24),
        cost_estimate=cost(6 * 4 * HALF * TOK * 256, 8 << 20),
        name="attend_near",
    )(table, own, *packs)


def attend_far(table, own, x2, turned, state):
    return pl.pallas_call(
        far_kernel,
        out_shape=arrays([((2, HALF, 128), F32)] * 2 + BACK * 3),
        in_specs=[SM, SM, ANY, ANY] + [VM] * 6,
        out_specs=(VM,) * 5,
        scratch_shapes=scratch(STATE + SLOTS + QPACKS) + SEMS + scratch(TILE),
        compiler_params=params(30),
        cost_estimate=cost(10 * 4 * HALF * TOK * 256, 8 << 20),
        name="attend_far",
    )(table, own, x2, turned, *state)


def combine_kernel(own, o_own, lse_own, x1, x2, x3, u, w, out):
    z = own[0] // SIDE
    high = z >= 2
    backs = ((x1, high), (x2, high), (x3, high), (u, z % 2 == 1), (w, high))
    for half in range(2):
        base = BACK_ROWS * half
        lses = []
        for back, there in backs:
            tail = back[base + HALF : base + BACK_ROWS, :].astype(F32)
            lses.append(jnp.where(there, tail[0:4] + tail[4:8] + tail[8:12], LOW))
        for b in range(4):
            rows = slice(128 * b, 128 * b + 128)
            columns = [lse_own[half, rows, :]]
            columns += [jnp.broadcast_to(to_column(v[b : b + 1, :]), (128, 128)) for v in lses]
            most = functools.reduce(jnp.maximum, columns)
            shares = [jnp.exp2(c - most) for c in columns]
            mixed = shares[0] * o_own[half, rows, :]
            for share, (back, _) in zip(shares[1:], backs):
                mixed = mixed + share * back[base + 128 * b : base + 128 * b + 128, :].astype(F32)
            out[4 * half + b] = (mixed / functools.reduce(jnp.add, shares)).astype(BF16)


def combine(own, o_own, lse_own, backs):
    return pl.pallas_call(
        combine_kernel,
        out_shape=jax.ShapeDtypeStruct((8, 128, 128), BF16),
        in_specs=[SM] + [VM] * 7,
        out_specs=VM,
        compiler_params=params(16),
        cost_estimate=cost(1 << 29, 2 << 20),
        name="combine",
    )(own, o_own, lse_own, *backs)


def conv_out_kernel(parts, w_hbm, out, later, rows, w, sems):
    copies = []
    for j in range(4):
        cols = pl.ds(512 * j, 512)
        copies.append(
            pltpu.make_async_copy(w_hbm.at[pl.ds(0, 1024), cols], w.at[:, cols], sems.at[j])
        )
    copies.append(pltpu.make_async_copy(w_hbm.at[pl.ds(1024, 1024)], later, sems.at[4]))
    for c in copies:
        c.start()
    total = functools.reduce(jnp.add, [parts[c, :128, :] for c in range(8)])
    mean = jnp.sum(total, axis=1, keepdims=True) * (1.0 / 1024)
    far = [parts[c, :128, :] - mean for c in range(8)]
    spread = functools.reduce(jnp.add, [v * v for v in far])
    spread = jnp.sum(spread, axis=1, keepdims=True) * (1.0 / 1024)
    inverse = lax.rsqrt(spread + EPS)
    for c in range(8):
        v = far[c] * inverse * parts[c, 128:129, :]
        rows[:, 128 * c : 128 * c + 128] = (v * jax.nn.sigmoid(v)).astype(BF16)
    for j in range(4):
        copies[j].wait()
        out[:, 512 * j : 512 * j + 512] = dot(rows[...], w[:, 512 * j : 512 * j + 512])
    copies[4].wait()


def conv_out(parts, w):
    return pl.pallas_call(
        conv_out_kernel,
        out_shape=(
            jax.ShapeDtypeStruct((128, 2048), F32),
            jax.ShapeDtypeStruct((1024, 2048), BF16),
        ),
        in_specs=[VM, HBM],
        out_specs=(VM, VM),
        scratch_shapes=[
            pltpu.VMEM((128, 1024), BF16),
            pltpu.VMEM((1024, 2048), BF16),
            pltpu.SemaphoreType.DMA((5,)),
        ],
        compiler_params=params(14),
        cost_estimate=cost(2 * 128 * 1024 * 2048 * 4, 6 << 20),
        name="conv_out",
    )(parts, w)


def attn_out_kernel(parts, conv, w, out, rows):
    for c in range(8):
        rows[:, 128 * c : 128 * c + 128] = parts[c]
    for j in range(4):
        cols = slice(512 * j, 512 * j + 512)
        out[:, cols] = (dot(rows[...], w[:, cols]) + conv[:, cols]).astype(BF16)


def attn_out(parts, conv, w):
    return pl.pallas_call(
        attn_out_kernel,
        out_shape=jax.ShapeDtypeStruct((128, 2048), BF16),
        in_specs=[VM, VM, VM],
        out_specs=VM,
        scratch_shapes=[pltpu.VMEM((128, 1024), BF16)],
        compiler_params=params(10),
        cost_estimate=cost(2 * 128 * 1024 * 2048 * 4, 6 << 20),
        name="attn_out",
    )(parts, conv, w)


def levels(*pairs):
    return [(a * SIDE + x, b * SIDE + x) for a, b in pairs for x in range(SIDE)]


def along_x(d):
    return [(z * SIDE + x, z * SIDE + (x + d) % SIDE) for z in (2, 3) for x in range(SIDE)]


def layer(x, wq, wk, wv, wu, wg, taps, gain, gate, w_out):
    x, wq, wk, wv, wu, wg, w_out = (
        pltpu.with_memory_space_constraint(v, pltpu.HBM) for v in (x, wq, wk, wv, wu, wg, w_out)
    )
    own = lax.axis_index("sp").astype(I32).reshape(1)
    table = jnp.asarray(work_table())
    pkv, pxx, pr, pq, gated, tail = project(own, x, wq, wk, wv, wu, wg, in_hbm(gate.reshape(8, 128)))
    halo = lax.ppermute(tail, "sp", [(i, i + 1) for i in range(15)])
    x1 = lax.ppermute(pxx, "sp", moves(-1, 0))
    x3 = lax.ppermute(pxx, "sp", moves(-3, 0))
    turned = lax.ppermute(pr, "sp", levels((0, 2), (2, 3), (3, 1), (1, 0)))
    swapped = lax.ppermute(pxx, "sp", levels((0, 3), (1, 2), (2, 1), (3, 0)))
    x2 = lax.ppermute(pxx, "sp", moves(-2, 0))
    conv = convolve(gated, halo, taps, gain.reshape(1, 128))
    conv_parts = lax.all_to_all(conv, "tp", 0, 0, tiled=True)
    near = (in_hbm(pkv), in_hbm(pq), x1, x3, swapped)
    state = attend_near(table, own, *near)
    far = attend_far(table, own, x2, turned, state)
    o_own, lse_own, b1, b2, b3 = far
    back1 = lax.ppermute(b1, "sp", along_x(1))
    back3 = lax.ppermute(b3, "sp", along_x(3))
    back2 = lax.ppermute(b2, "sp", along_x(2))
    back_u = lax.ppermute(b1, "sp", levels((0, 1), (1, 3)))
    back_w = lax.ppermute(b2, "sp", levels((1, 2), (0, 3)))
    conv_mixed, w_attn = conv_out(conv_parts, w_out)
    mixed = combine(own, o_own, lse_own, (back1, back2, back3, back_u, back_w))
    attn_parts = lax.all_to_all(mixed, "tp", 0, 0, tiled=True)
    return attn_out(attn_parts, conv_mixed, w_attn)


def in_hbm(value):
    return pltpu.with_memory_space_constraint(value, pltpu.HBM)


def solution(mesh):
    in_specs = (
        P("sp", None),
        P(None, "tp"),
        P(None, "tp"),
        P(None, "tp"),
        P(None, "tp"),
        P(None, "tp"),
        P(None, "tp"),
        P("tp"),
        P("sp", "tp"),
        P(),
    )
    out_specs = P(("sp", "tp"), None)
    return jax.shard_map(layer, mesh=mesh, in_specs=in_specs, out_specs=out_specs, check_vma=False)
```
